32 devices in a mesh: fs: 4 (over y, x), tp: 8 (over z, core).
Axes of the slice: x: 2, y: 2, z: 4, core: 2. Of those that a mesh axis runs over, the one named last changes fastest.
Arguments:
- tokens: bfloat16 [1024, 2048], P('fs', 'tp'), may hold values from -60 to 60
- norm_gain: float32 [2048], P('fs'), may hold values from 0.1 to 1.9
- gate_weight: float32 [4, 2048, 4096], P(None, 'fs', 'tp'), may hold values from -0.125 to 0.125
- up_weight: float32 [4, 2048, 4096], P(None, 'fs', 'tp'), may hold values from -0.125 to 0.125
- down_weight: float32 [4, 2048, 4096], P(None, 'fs', 'tp'), may hold values from -0.125 to 0.125
- route: int32 [1024, 2], P('fs'), may hold values from 0 to 3, all different within a row; in each aligned block of 256 rows (0 to 255, 256 to 511, ...) at most 256 rows name the same one
- route_weight: float32 [1024, 2], P('fs'), may hold values from 0.2 to 1
Outputs:
- mixed: bfloat16 [1024, 2048], P('fs', 'tp')
- gate_new: bfloat16 [4, 2048, 4096], P('fs', None, 'tp')
- up_new: bfloat16 [4, 2048, 4096], P('fs', None, 'tp')
- down_new: bfloat16 [4, 2048, 4096], P('fs', None, 'tp')
The draws below stay inside these ranges and needn't reach their ends.
Inputs may be any that keep to these rules, and one draw needn't show every extreme that they name: `route`: the 2 experts of a row differ. In each aligned block of 256 rows (the tokens of one index of fs) no expert is named by more than 256 rows, a bound that some block reaches.
All inputs are finite; a program needn't handle non-finite values.
Results may differ from the reference program's by a relative error of at most 0.024.
Values may be sent and summed in bfloat16 or wider, within the bound.
A program may use at most 64 MiB of HBM per device.

```python
import math
import jax
import jax.numpy as jnp
import numpy as np
from jax import lax

D = 2048
FF = 4096
TOP = 2
TOK_DEV = 256
EXPERTS = 4
CAP = 256
TOKENS = 1024
N_FS = 4
N_TP = 8


def draw_tokens(key, part):
    key_base = jax.random.fold_in(key, 11)
    values = jax.random.normal(key_base, (TOKENS, D), jnp.float32)
    column_scale = 0.6 * 3.0 ** (jnp.arange(D, dtype=jnp.float32) / D)
    values = jnp.clip(values * column_scale[None, :], -60.0, 60.0)
    return values.astype(jnp.bfloat16)


def strengthened(result, own_key, source, target, parts, factor):
    def block_of(dim):
        return (jnp.arange(result.shape[dim]) // (result.shape[dim] // parts)).reshape((-1,) + (1,) * (result.ndim - 1 - dim))

    first = jax.random.permutation(own_key, parts)[block_of(target)]
    other_side = (block_of(target) + parts // 2) % parts
    return jnp.where((block_of(source) == first) | (block_of(source) == other_side), factor * result, result)


def block_levels(rng, extent, cuts, least, top_value):
    gain = 1.0
    for dim, blocks in cuts:
        heights = jax.random.uniform(jax.random.fold_in(jax.random.fold_in(rng, 6), dim), (blocks,), jnp.float32, least / len(cuts), top_value / len(cuts))
        gain = gain * jnp.repeat(jnp.exp(heights), extent[dim] // blocks).reshape((-1,) + (1,) * (len(extent) - 1 - dim))
    return gain


def assign_block(stream_key, own, number, rows, amount, top, bound, slope):
    ranking = jax.random.permutation(stream_key, amount)
    heavy_load, ordinary = portions_of(amount, rows * top, bound, slope, True), portions_of(amount, rows * top, bound, slope, False)
    places = jnp.arange(amount)

    def named(tallies, offset_by):
        used = int((tallies > 0).sum())
        fixed = max(1, used // 4)
        moved = fixed + (places - fixed + offset_by * (used - fixed)) % max(1, amount - fixed)
        return jnp.zeros((amount,), jnp.int32).at[ranking[jnp.where(places < fixed, places, moved)]].set(jnp.asarray(tallies, jnp.int32))

    tallies = jnp.where(number % 4 == 0, named(heavy_load, number // 4), named(ordinary, number - number // 4 - 1))
    mixed = jax.random.permutation(jax.random.fold_in(own, 3), amount)
    donor, receiver = mixed[0:amount // 2 * 2:2], mixed[1:amount // 2 * 2:2]
    slack = jnp.minimum(tallies[donor] - 1, bound - tallies[receiver]) // 2
    slack = jnp.where((donor == ranking[0]) | (receiver == ranking[0]) | (tallies[receiver] == 0), 0, jnp.maximum(slack, 0))
    moved = jax.random.randint(jax.random.fold_in(own, 4), (amount // 2,), 0, 1 << 20) % (slack + 1)
    tallies = tallies.at[donor].add(-moved).at[receiver].add(moved)
    members = jnp.searchsorted(jnp.cumsum(tallies), jnp.arange(rows * top), side="right").astype(jnp.int32)
    table = members.reshape(top, rows).T
    table = table[jax.random.permutation(jax.random.fold_in(own, 1), rows)]
    offset_by = jax.random.randint(jax.random.fold_in(own, 2), (rows, 1), 0, top)
    return jnp.take_along_axis(table, (jnp.arange(top)[None, :] + offset_by) % top, axis=1)


def portions_of(amount, total, reach, skew, full):
    weights = [(1 << 20) // math.isqrt(grade ** skew) + 1 for grade in range(1, amount + 1)]
    largest = reach if full else min(reach, max(-(-total // amount), total * weights[0] // sum(weights)))
    least = 1 if total - largest >= amount - 1 else 0
    given, spare = [largest] + [least] * (amount - 1), total - largest - least * (amount - 1)
    while spare > 0:
        candidates = [i for i in range(1, amount) if given[i] < largest] or [i for i in range(1, amount) if given[i] < reach]
        pool, remaining = sum([weights[i] for i in candidates]), spare
        for i in candidates:
            more = min(reach - given[i], max(1, remaining * weights[i] // pool), spare)
            given[i] = given[i] + more
            spare = spare - more
    return np.array(given)


def noise(rng, dims, spread, bound, pieces=(), kind=jnp.bfloat16):
    factor_of = block_levels(rng, dims, pieces, -0.22, 0.18) if pieces else 1.0
    entries = jax.random.normal(rng, dims, jnp.float32) * spread * factor_of
    return jnp.minimum(jnp.maximum(entries, -bound), bound).astype(kind)


def gaussian_with(stream_key, extent, spread, most, split, heavy, kind=jnp.bfloat16):
    drawn = spread * jax.random.normal(stream_key, extent, jnp.float32)
    if split:
        drawn = drawn * block_levels(stream_key, extent, split, -0.22, 0.18)
    return jnp.clip(strengthened(drawn, jax.random.fold_in(stream_key, 3), *heavy), -most, most).astype(kind)


def setup_inputs(seed: int = 0) -> dict:
    streams_of = jax.random.split(jax.random.key(seed), 8)
    tokens = draw_tokens(jax.random.fold_in(streams_of[7], 71), 0)
    norm_gain = jnp.clip(1.0 + 0.18 * jax.random.normal(streams_of[1], (D,), jnp.float32), 0.1, 1.9)
    gate_weight = noise(streams_of[2], (EXPERTS, D, FF), D ** -0.5, 0.125, ((1, 4), (2, 8)), jnp.float32)
    up_weight = noise(streams_of[3], (EXPERTS, D, FF), D ** -0.5, 0.125, ((1, 4), (2, 8)), jnp.float32)
    down_weight = gaussian_with(streams_of[4], (EXPERTS, D, FF), FF ** -0.5, 0.125, ((1, 4), (2, 8)), (2, 1, 8, 2.0), jnp.float32)
    route_keys = jax.random.split(jax.random.fold_in(streams_of[5], 1), TOKENS // TOK_DEV)
    route_turns = jax.random.permutation(jax.random.fold_in(streams_of[5], 3), TOKENS // TOK_DEV)
    route = jax.vmap(lambda own, number: assign_block(jax.random.fold_in(streams_of[5], 2), own, number, TOK_DEV, EXPERTS, TOP, CAP, 2))(route_keys, route_turns).reshape((TOKENS, TOP))
    route_weight = jnp.clip(jnp.exp(math.log(1.0) - 1.609438 * jax.random.uniform(streams_of[6], (TOKENS, TOP), jnp.float32) ** block_levels(streams_of[6], (TOKENS, TOP), ((0, 4),), -0.2, 0.2)), 0.2, 1.0)
    return {"tokens": tokens, "norm_gain": norm_gain, "gate_weight": gate_weight, "up_weight": up_weight, "down_weight": down_weight, "route": route, "route_weight": route_weight}


epsilon = 1e-05

def slot_table(route, block_rows, expert_count):
    pair_ids = route.reshape(-1, block_rows * route.shape[1])
    onehot = (pair_ids[:, :, None] == jnp.arange(expert_count, dtype=jnp.int32)[None, None, :]).astype(jnp.int32)
    before = jnp.cumsum(onehot, axis=1) - onehot
    return lax.optimization_barrier(jnp.sum(before * onehot, axis=2)).astype(jnp.int32).reshape(route.shape)

def reference(tokens, norm_gain, gate_weight, up_weight, down_weight, route, route_weight):
    gain_col = norm_gain.astype(jnp.float32)[None, :, None]
    gate_new = (gate_weight * gain_col).astype(jnp.bfloat16)
    up_new = (up_weight * gain_col).astype(jnp.bfloat16)
    down_new = down_weight.astype(jnp.bfloat16)
    tok_float = tokens.astype(jnp.float32)
    normed = (tok_float * lax.rsqrt(lax.optimization_barrier(jnp.mean(tok_float * tok_float, axis=1, keepdims=True)) + epsilon)).astype(jnp.bfloat16)
    slot_of = slot_table(route, TOK_DEV, EXPERTS)
    groups = jnp.broadcast_to((jnp.arange(TOKENS, dtype=jnp.int32) // TOK_DEV)[:, None], route.shape)
    token_index = jnp.broadcast_to(jnp.arange(TOKENS, dtype=jnp.int32)[:, None], route.shape)
    row_table = jnp.full((EXPERTS, N_FS, CAP), TOKENS, jnp.int32).at[route, groups, slot_of].set(token_index)
    padded = jnp.concatenate([normed, jnp.zeros((1, D), jnp.bfloat16)], axis=0)
    block_width = FF // N_TP

    def one_expert(operands):
        gate_e, up_e, down_e, rows_e = operands
        expert_rows = padded[rows_e.reshape(-1)]
        gate_acc = jnp.dot(expert_rows, gate_e, preferred_element_type=jnp.float32)
        up_acc = jnp.dot(expert_rows, up_e, preferred_element_type=jnp.float32)
        hidden = (jax.nn.silu(gate_acc) * up_acc).astype(jnp.bfloat16)

        def add_block(block, running):
            offset = jnp.asarray(block, jnp.int32) * block_width
            part_hidden = lax.dynamic_slice_in_dim(hidden, offset, block_width, 1)
            part_weight = lax.dynamic_slice_in_dim(down_e, offset, block_width, 1)
            term = lax.dot_general(part_hidden, part_weight, (((1,), (1,)), ((), ())), preferred_element_type=jnp.float32)
            return running + term.astype(jnp.bfloat16).astype(jnp.float32)
        summed = lax.fori_loop(0, N_TP, add_block, jnp.zeros((N_FS * CAP, D), jnp.float32))
        return summed.astype(jnp.bfloat16)
    outputs = lax.map(one_expert, (gate_new, up_new, down_new, row_table))
    flat = outputs.reshape(EXPERTS * N_FS * CAP, D)
    index = ((route * N_FS + groups) * CAP + slot_of).astype(jnp.int32)
    picked = flat[index].astype(jnp.float32)
    mixed = lax.optimization_barrier(jnp.sum(picked * route_weight.astype(jnp.float32)[:, :, None], axis=1)).astype(jnp.bfloat16)
    return (mixed, gate_new, up_new, down_new)
```

```python
import functools

import jax
import jax.numpy as jnp
from jax import lax
from jax.experimental import pallas as pl
from jax.experimental.pallas import tpu as pltpu
from jax.sharding import PartitionSpec as P

epsilon = 1e-05


def slot_table(route, block_rows, expert_count):
    pair_ids = route.reshape(-1, block_rows * route.shape[1])
    onehot = (
        pair_ids[:, :, None] == jnp.arange(expert_count, dtype=jnp.int32)[None, None, :]
    ).astype(jnp.int32)
    before = jnp.cumsum(onehot, axis=1) - onehot
    return jnp.sum(before * onehot, axis=2).reshape(route.shape)


def slotted_body(tokens, norm_gain, gate_weight, up_weight, down_weight, route, route_weight):
    experts = gate_weight.shape[0]
    tok_rows = tokens.shape[0]
    columns = tokens.shape[1]
    fs_count = lax.axis_size("fs")
    capacity = 4 * tok_rows // fs_count
    gain_col = norm_gain[None, :, None]
    gate_cast = (gate_weight * gain_col).astype(jnp.bfloat16)
    up_cast = (up_weight * gain_col).astype(jnp.bfloat16)
    down_cast = down_weight.astype(jnp.bfloat16)
    gate_new, up_new, down_new = (
        lax.all_to_all(gate_cast, "fs", split_axis=0, concat_axis=1, tiled=True),
        lax.all_to_all(up_cast, "fs", split_axis=0, concat_axis=1, tiled=True),
        lax.all_to_all(down_cast, "fs", split_axis=0, concat_axis=1, tiled=True),
    )
    slot_of = slot_table(route, tok_rows, experts)
    target = route * capacity + slot_of
    slot_lanes = jnp.arange(experts * capacity, dtype=jnp.int32)
    slot_hits = target[:, :, None] == slot_lanes[None, None, :]
    token_iota = jnp.arange(tok_rows, dtype=jnp.int32)[:, None, None]
    lane_token = jnp.sum(jnp.where(slot_hits, token_iota + 1, 0), axis=(0, 1)) - 1
    lane_token = jnp.where(lane_token < 0, tok_rows, lane_token)
    combine = jnp.sum(jnp.where(slot_hits, route_weight[:, :, None], 0.0), axis=1)
    tok_float = tokens.astype(jnp.float32)
    square_sum = lax.psum(jnp.sum(tok_float * tok_float, axis=1), "tp")
    full_width = columns * lax.axis_size("tp")
    normed = (tok_float * lax.rsqrt(square_sum / full_width + epsilon)[:, None]).astype(
        jnp.bfloat16
    )
    padded = jnp.concatenate([normed, jnp.zeros((1, columns), jnp.bfloat16)], axis=0)
    outgoing = padded[lane_token].reshape(experts, capacity, columns)
    arrived = lax.all_to_all(outgoing, "fs", split_axis=0, concat_axis=0, tiled=True).reshape(
        -1, columns
    )
    gate_local = gate_new[0]
    up_local = up_new[0]
    piece_rows = lax.all_gather(arrived, "tp", axis=1, tiled=True)
    gate_acc = jnp.dot(piece_rows, gate_local, preferred_element_type=jnp.float32)
    up_acc = jnp.dot(piece_rows, up_local, preferred_element_type=jnp.float32)
    hidden = (jax.nn.silu(gate_acc) * up_acc).astype(jnp.bfloat16)
    down_local = down_new[0]
    summed = lax.psum_scatter(
        lax.dot_general(
            down_local, hidden, (((1,), (1,)), ((), ())), preferred_element_type=jnp.float32
        ).astype(jnp.bfloat16),
        "tp",
        scatter_dimension=0,
        tiled=True,
    ).astype(jnp.float32)
    own_columns = summed.shape[0]
    outgoing_back = summed.astype(jnp.bfloat16).reshape(own_columns, fs_count, capacity)
    returned = lax.all_to_all(outgoing_back, "fs", split_axis=1, concat_axis=1, tiled=True).reshape(
        own_columns, experts * capacity
    )
    mixed = lax.dot_general(
        combine,
        returned.astype(jnp.float32),
        (((1,), (1,)), ((), ())),
        precision=lax.Precision.HIGHEST,
        preferred_element_type=jnp.float32,
    )
    return (mixed.astype(jnp.bfloat16), gate_new, up_new, down_new)


MESH = pl.DeviceIdType.MESH
STAGES = 2
HALVES = 2
LAG = 2
ROW_TILE = 256
ISSUE = (3, 1, 2)
ARRIVE = (2, 3, 1)


def flip(index, distance):
    bit = 1
    while bit <= distance:
        if distance & bit:
            index = index + bit - 2 * bit * ((index // bit) % 2)
        bit *= 2
    return index


def rows_of(index, size):
    return pl.ds(pl.multiple_of(index * size, size), size)


def moe_kernel(
    fs,
    tp,
    tokens,
    gain,
    gate,
    up,
    down,
    route,
    route_weight,
    mixed,
    gate_out,
    up_out,
    down_out,
    loaded,
    staged,
    w_gate,
    w_up,
    w_down,
    tok,
    gated,
    up_acc,
    hidden,
    pair_own,
    pair_out,
    pair_in,
    chain_in,
    chain_out,
    back_in,
    share,
    mix_out,
    mix_in,
    gain_col,
    load_sem,
    tok_local,
    tf_s,
    tf_r,
    az_s,
    az_r,
    as_s,
    as_r,
    w_s,
    w_r,
    dn_s,
    dn_r,
    pr_s,
    pr_r,
    ch_s,
    ch_r,
    bk_s,
    bk_r,
    mx_s,
    mx_r,
    out_sem,
):
    chips = tp // 2
    last = chips - 1
    f = lax.axis_index("fs")
    t = lax.axis_index("tp")
    z, core = t // 2, t % 2
    sibling = flip(t, 1)
    onward = t + 4 * core - 2
    place = core * z + (1 - core) * (last - z)
    block, width = tokens.shape
    depth, units = gate.shape[1], gate.shape[2]
    sub = width // STAGES
    half = fs * block // HALVES
    sources, finals = (gate, up, down), (w_gate, w_up, w_down)

    barrier = pltpu.get_barrier_semaphore()
    for d in range(1, fs):
        pl.semaphore_signal(barrier, inc=1, device_id={"fs": flip(f, d)}, device_id_type=MESH)
    near = [1] + list(range(2, tp, 2))
    for d in near:
        pl.semaphore_signal(barrier, inc=1, device_id={"tp": flip(t, d)}, device_id_type=MESH)

    def tok_at(k, d):
        return tok.at[k, rows_of(flip(f, d), block)]

    own_tok = pltpu.make_async_copy(tokens, tok_at(t, 0), tok_local)
    own_tok.start()
    loads = {}

    def load(p, d):
        loads[p, d] = pltpu.make_async_copy(
            sources[p].at[flip(f, d)], loaded.at[p, d], load_sem.at[p, d]
        )
        loads[p, d].start()

    for d in ISSUE:
        load(0, d)
    gain_col[...] = jnp.broadcast_to(gain[...], (128, depth)).T
    own_tok.wait()
    pl.semaphore_wait(barrier, fs - 1 + len(near))

    pending = []

    def remote(src, dst, s_sem, r_sem, **device):
        return pltpu.make_async_remote_copy(
            src_ref=src,
            dst_ref=dst,
            send_sem=s_sem,
            recv_sem=r_sem,
            device_id=device,
            device_id_type=MESH,
        )

    def send(*args, **device):
        copy = remote(*args, **device)
        copy.start()
        pending.append((None, copy))
        return copy

    def send_if(condition, *args, **device):
        @pl.when(condition)
        def _():
            remote(*args, **device).start()

        pending.append((condition, (args, device)))

    tok_fs = {
        d: send(tok_at(t, 0), tok_at(t, 0), tf_s.at[d], tf_r.at[d], fs=flip(f, d)) for d in ISSUE
    }

    def spread(d):
        piece = tok_at(t, d)
        send_if(z < last, piece, piece, az_s.at[0, 0, d], az_r.at[z, d], tp=t + 2)
        send_if(z > 0, piece, piece, az_s.at[1, 0, d], az_r.at[z, d], tp=t - 2)
        send(piece, piece, as_s.at[0, 0, d], as_r.at[z, d], tp=sibling)

    def relay(step, d):
        for way in range(2):
            towards = 1 - 2 * way
            here = (z >= step) if way == 0 else (z + step <= last)
            more = (z < last) if way == 0 else (z > 0)
            k = t - 2 * step * towards
            origin = z - step * towards
            piece = tok_at(k, d)

            @pl.when(here)
            def _():
                remote(
                    piece, piece, az_s.at[way, step, d], az_r.at[origin, d], tp=sibling
                ).wait_recv()

            send_if(
                jnp.logical_and(here, more),
                piece,
                piece,
                az_s.at[way, step, d],
                az_r.at[origin, d],
                tp=t + 2 * towards,
            )
            send_if(here, piece, piece, as_s.at[way, step, d], as_r.at[origin, d], tp=sibling)

    def cast(p, d):
        loads[p, d].wait()
        tile = 64

        @pl.loop(0, depth // tile)
        def _(i):
            rows = rows_of(i, tile)
            value = loaded[p, d, rows, :]
            if p < 2:
                value = value * gain_col[rows, 0:1]
            value = value.astype(jnp.bfloat16)
            if d:
                staged[p, d - 1, rows, :] = value
            else:
                finals[p][pl.ds(pl.multiple_of(f * depth + i * tile, tile), tile), :] = value

    arrive = {}

    def ship(p, d):
        cast(p, d)
        arrive[p, d] = send(
            staged.at[p, d - 1],
            finals[p].at[rows_of(f, depth)],
            w_s.at[p, d],
            w_r.at[p, d],
            fs=flip(f, d),
        )

    spread(0)
    for d in ISSUE:
        load(1, d)
    for d in ISSUE:
        ship(0, d)
    for d in ISSUE:
        load(2, d)
    for d in ISSUE:
        tok_fs[d].wait_recv()
        spread(d)
    for d in ISSUE:
        ship(1, d)
    for p in range(3):
        load(p, 0)
    for d in ISSUE:
        cast(2, d)
    for u in range(STAGES):
        for d in ISSUE:
            for c in range(2):
                arrive[2, u, d, c] = send(
                    staged.at[2, d - 1, pl.ds(c * width + u * sub, sub)],
                    w_down.at[
                        pl.ds(pl.multiple_of(f * depth + (c * width + u * sub), sub), sub)
                    ],
                    dn_s.at[u, d, c],
                    dn_r.at[u, d, c],
                    fs=flip(f, d),
                )
    for step in range(1, chips):
        for d in (0,) + ISSUE:
            relay(step, d)
        if step == 1:
            for p in range(3):
                cast(p, 0)
            for e in range(fs):
                part = jnp.zeros((1, block), jnp.float32)
                for k in range(route.shape[0]):
                    part = part + jnp.where(
                        route[k : k + 1, :] == e, route_weight[k : k + 1, :], 0.0
                    )
                share[e] = jnp.broadcast_to(part, (sub, block)).T
    for origin in range(chips):
        for d in (0,) + ISSUE:
            piece = tok_at(2 * origin + 1 - core, d)
            remote(
                piece, piece, as_s.at[0, 0, d], as_r.at[origin, d], tp=sibling
            ).wait_recv()

    for d in ISSUE:
        arrive[0, d].wait_recv()
    outs = [
        pltpu.make_async_copy(w_gate, gate_out, out_sem.at[0]),
        pltpu.make_async_copy(w_up, up_out, out_sem.at[1]),
        pltpu.make_async_copy(w_down, down_out, out_sem.at[2]),
    ]
    outs[0].start()

    @pl.loop(0, fs * block // ROW_TILE)
    def _(i):
        rows = rows_of(i, ROW_TILE)
        parts = [tok[k, rows, :] for k in range(tp)]
        squares = jnp.zeros((ROW_TILE, 1), jnp.float32)
        for part in parts:
            value = part.astype(jnp.float32)
            squares = squares + jnp.sum(value * value, axis=1, keepdims=True)
        scale = lax.rsqrt(squares / (width * tp) + epsilon)
        acc = jnp.dot(
            jnp.concatenate(parts, axis=1), w_gate[...], preferred_element_type=jnp.float32
        )
        gated[rows, :] = jax.nn.silu(acc * scale) * scale

    def up_part(d, rows):
        s = flip(f, d)
        value = jnp.concatenate([tok[2 * s, rows, :], tok[2 * s + 1, rows, :]], axis=1)
        return jnp.dot(value, w_up[rows_of(s, depth), :], preferred_element_type=jnp.float32)

    early = (0,) + ARRIVE[:-1]
    for n, d in enumerate(early):
        if d:
            arrive[1, d].wait_recv()

        @pl.loop(0, fs * block // ROW_TILE)
        def _(i):
            rows = rows_of(i, ROW_TILE)
            part = up_part(d, rows)
            up_acc[rows, :] = up_acc[rows, :] + part if n else part

    arrive[1, ARRIVE[-1]].wait_recv()

    @pl.loop(0, fs * block // ROW_TILE)
    def _(i):
        rows = rows_of(i, ROW_TILE)
        value = up_acc[rows, :] + up_part(ARRIVE[-1], rows)
        hidden[rows, :] = (gated[rows, :] * value).astype(jnp.bfloat16)

    outs[1].start()

    items = [(u, 0) for u in range(STAGES)]
    items += [(u, d) for u in range(STAGES) for d in ARRIVE]
    pieces = [(u, d, h) for u, d in items for h in range(HALVES)]
    count = len(pieces)

    def product(q):
        u, d, h = pieces[q]
        s = flip(f, d)
        if d and h == 0:
            for c in range(2):
                arrive[2, u, d, c].wait_recv()

        def weights(c):
            start = pl.multiple_of(s * depth + c * width + u * sub, sub)
            return w_down[pl.ds(start, sub), :]

        @pl.loop(0, half // ROW_TILE)
        def _(i):
            rows = rows_of(i, ROW_TILE)
            value = hidden[pl.ds(pl.multiple_of(h * half + i * ROW_TILE, ROW_TILE), ROW_TILE), :]
            result = lax.dot_general(
                value,
                jnp.concatenate([weights(core), weights(1 - core)], axis=0),
                (((1,), (1,)), ((), ())),
                preferred_element_type=jnp.float32,
            )
            pair_own[q, rows, :] = result[:, :sub]
            pair_out[q, rows, :] = result[:, sub:].astype(jnp.bfloat16)

        send(pair_out.at[q], pair_in.at[q], pr_s.at[q], pr_r.at[q], tp=sibling)

    per_half = half // block

    def advance(p, j):
        u, d, h = pieces[j]
        s = flip(f, d)
        remote(
            pair_out.at[j], pair_in.at[j], pr_s.at[j], pr_r.at[j], tp=sibling
        ).wait_recv()
        onto = (chain_out.at[j], chain_in.at[j], ch_s.at[j], ch_r.at[j])
        if p:
            remote(*onto, tp=sibling).wait_recv()

        @pl.loop(0, half // ROW_TILE)
        def _(i):
            rows = rows_of(i, ROW_TILE)
            value = pair_own[j, rows, :] + pair_in[j, rows, :].astype(jnp.float32)
            if p:
                value = value + chain_in[j, rows, :].astype(jnp.float32)
            chain_out[j, rows, :] = value.astype(jnp.bfloat16)

        if p < last:
            remote(*onto, tp=onward).start()
            return
        for n in range(per_half):
            b = h * per_half + n
            rows = pl.ds(n * block, block)

            @pl.when(f != b)
            def _():
                remote(
                    chain_out.at[j, rows],
                    back_in.at[u, s, f],
                    bk_s.at[j, n],
                    bk_r.at[u, s, f],
                    fs=b,
                ).start()

            @pl.when(f == b)
            def _():
                back_in[u, s, f] = chain_out[j, rows, :]

    def combine(u):
        for e in range(fs):

            @pl.when(e != f)
            def _():
                for s in range(fs):
                    remote(
                        back_in.at[u, s, e],
                        back_in.at[u, s, e],
                        bk_s.at[0, 0],
                        bk_r.at[u, s, e],
                        fs=flip(f, 1),
                    ).wait_recv()

        for s in range(fs):
            value = jnp.zeros((block, sub), jnp.float32)
            for e in range(fs):
                value = value + share[e] * back_in[u, s, e].astype(jnp.float32)
            value = value.astype(jnp.bfloat16)

            @pl.when(s == z)
            def _():
                mix_in[u] = value

            @pl.when(s != z)
            def _():
                mix_out[u, s] = value
                remote(
                    mix_out.at[u, s], mix_in.at[u], mx_s.at[u, s], mx_r.at[u], tp=2 * s + core
                ).start()

    ready = {}
    for u in range(STAGES):
        done = max(j for j in range(count) if pieces[j][0] == u) + 1 + LAG * last
        ready[min(done + 1, count + LAG * last)] = ready.get(
            min(done + 1, count + LAG * last), []
        ) + [u]
    for q in range(count + 1 + LAG * last):
        if q < count:
            product(q)
        if q == count:
            outs[2].start()
        for p in range(chips):
            j = q - 1 - LAG * p
            if 0 <= j < count:

                @pl.when(place == p)
                def _():
                    advance(p, j)

        for u in ready.get(q, []):

            @pl.when(place == last)
            def _():
                combine(u)

    @pl.when(place < last)
    def _():
        for u in range(STAGES):
            remote(
                mix_out.at[u, 0], mix_in.at[u], mx_s.at[u, 0], mx_r.at[u], tp=sibling
            ).wait_recv()

    for u in range(STAGES):
        mixed[:, u * sub : (u + 1) * sub] = mix_in[u]

    for condition, copy in pending:
        if condition is None:
            copy.wait_send()
        else:

            @pl.when(condition)
            def _():
                args, device = copy
                remote(*args, **device).wait_send()

    @pl.when(place < last)
    def _():
        for j in range(count):
            remote(
                chain_out.at[j], chain_in.at[j], ch_s.at[j], ch_r.at[j], tp=sibling
            ).wait_send()

    @pl.when(place == last)
    def _():
        for j in range(count):
            u, d, h = pieces[j]
            for n in range(per_half):
                b = h * per_half + n

                @pl.when(f != b)
                def _():
                    remote(
                        chain_out.at[j, pl.ds(n * block, block)],
                        back_in.at[u, 0, f],
                        bk_s.at[j, n],
                        bk_r.at[u, 0, f],
                        fs=b,
                    ).wait_send()

        for u in range(STAGES):
            for s in range(fs):

                @pl.when(s != z)
                def _():
                    remote(
                        mix_out.at[u, s], mix_in.at[u], mx_s.at[u, s], mx_r.at[u], tp=sibling
                    ).wait_send()

    for copy in outs:
        copy.wait()


def dense_body(tokens, norm_gain, gate_weight, up_weight, down_weight, route, route_weight):
    fs, tp = lax.axis_size("fs"), lax.axis_size("tp")
    block, width = tokens.shape
    experts, depth, units = gate_weight.shape
    rows, full, sub, chips = fs * block, tp * width, width // STAGES, tp // 2
    count, half = STAGES * fs * HALVES, rows // HALVES
    whole = pl.BlockSpec(memory_space=pltpu.VMEM)
    far = pl.BlockSpec(memory_space=pl.ANY)
    narrow, wide, dma = jnp.bfloat16, jnp.float32, pltpu.SemaphoreType.DMA
    weight = jax.ShapeDtypeStruct((full, units), narrow)
    mixed, gate_new, up_new, down_new = pl.pallas_call(
        functools.partial(moe_kernel, fs, tp),
        out_shape=(jax.ShapeDtypeStruct((block, width), narrow), weight, weight, weight),
        in_specs=[far, whole, far, far, far, whole, whole],
        out_specs=(whole, far, far, far),
        scratch_shapes=[
            pltpu.VMEM((3, experts, depth, units), wide),
            pltpu.VMEM((3, fs - 1, depth, units), narrow),
            pltpu.VMEM((full, units), narrow),
            pltpu.VMEM((full, units), narrow),
            pltpu.VMEM((full, units), narrow),
            pltpu.VMEM((tp, rows, width), narrow),
            pltpu.VMEM((rows, units), wide),
            pltpu.VMEM((rows, units), wide),
            pltpu.VMEM((rows, units), narrow),
            pltpu.VMEM((count, half, sub), wide),
            pltpu.VMEM((count, half, sub), narrow),
            pltpu.VMEM((count, half, sub), narrow),
            pltpu.VMEM((count, half, sub), narrow),
            pltpu.VMEM((count, half, sub), narrow),
            pltpu.VMEM((STAGES, fs, fs, block, sub), narrow),
            pltpu.VMEM((fs, block, sub), wide),
            pltpu.VMEM((STAGES, fs, block, sub), narrow),
            pltpu.VMEM((STAGES, block, sub), narrow),
            pltpu.VMEM((depth, 128), wide),
            dma((3, experts)),
            dma,
            dma((fs,)),
            dma((fs,)),
            dma((2, chips, fs)),
            dma((chips, fs)),
            dma((2, chips, fs)),
            dma((chips, fs)),
            dma((2, fs)),
            dma((2, fs)),
            dma((STAGES, fs, 2)),
            dma((STAGES, fs, 2)),
            dma((count,)),
            dma((count,)),
            dma((count,)),
            dma((count,)),
            dma((count, fs // HALVES)),
            dma((STAGES, fs, fs)),
            dma((STAGES, fs)),
            dma((STAGES,)),
            dma((3,)),
        ],
        compiler_params=pltpu.CompilerParams(
            collective_id=0, has_side_effects=True, vmem_limit_bytes=64000 * 1024
        ),
    )(tokens, norm_gain[None, :], gate_weight, up_weight, down_weight, route.T, route_weight.T)
    return mixed, gate_new[None], up_new[None], down_new[None]


def body(tokens, norm_gain, gate_weight, up_weight, down_weight, route, route_weight):
    fs, tp = lax.axis_size("fs"), lax.axis_size("tp")
    fits = (
        fs == 4
        and tp == 2 * fs
        and gate_weight.shape[0] == fs
        and tokens.shape[1] % (128 * STAGES) == 0
        and tokens.shape[0] % ROW_TILE == 0
        and gate_weight.shape[1] == 2 * tokens.shape[1]
        and tokens.shape[0] * fs * tokens.shape[1] * tp <= 1024 * 2048
    )
    chosen = dense_body if fits else slotted_body
    return chosen(tokens, norm_gain, gate_weight, up_weight, down_weight, route, route_weight)


def solution(mesh):
    in_specs = (
        P("fs", "tp"),
        P("fs"),
        P(None, "fs", "tp"),
        P(None, "fs", "tp"),
        P(None, "fs", "tp"),
        P("fs", None),
        P("fs", None),
    )
    out_specs = (P("fs", "tp"), P("fs", None, "tp"), P("fs", None, "tp"), P("fs", None, "tp"))
    return jax.shard_map(body, mesh=mesh, in_specs=in_specs, out_specs=out_specs, check_vma=False)
```

```python
import functools

import jax
import jax.numpy as jnp
from jax import lax
from jax.experimental import pallas as pl
from jax.experimental.pallas import tpu as pltpu
from jax.sharding import PartitionSpec as P

epsilon = 1e-05


def slot_table(route, block_rows, expert_count):
    pair_ids = route.reshape(-1, block_rows * route.shape[1])
    onehot = (
        pair_ids[:, :, None] == jnp.arange(expert_count, dtype=jnp.int32)[None, None, :]
    ).astype(jnp.int32)
    before = jnp.cumsum(onehot, axis=1) - onehot
    return jnp.sum(before * onehot, axis=2).reshape(route.shape)


def slotted_body(tokens, norm_gain, gate_weight, up_weight, down_weight, route, route_weight):
    experts = gate_weight.shape[0]
    tok_rows = tokens.shape[0]
    columns = tokens.shape[1]
    fs_count = lax.axis_size("fs")
    capacity = 4 * tok_rows // fs_count
    gain_col = norm_gain[None, :, None]
    gate_cast = (gate_weight * gain_col).astype(jnp.bfloat16)
    up_cast = (up_weight * gain_col).astype(jnp.bfloat16)
    down_cast = down_weight.astype(jnp.bfloat16)
    gate_new, up_new, down_new = (
        lax.all_to_all(gate_cast, "fs", split_axis=0, concat_axis=1, tiled=True),
        lax.all_to_all(up_cast, "fs", split_axis=0, concat_axis=1, tiled=True),
        lax.all_to_all(down_cast, "fs", split_axis=0, concat_axis=1, tiled=True),
    )
    slot_of = slot_table(route, tok_rows, experts)
    target = route * capacity + slot_of
    slot_lanes = jnp.arange(experts * capacity, dtype=jnp.int32)
    slot_hits = target[:, :, None] == slot_lanes[None, None, :]
    token_iota = jnp.arange(tok_rows, dtype=jnp.int32)[:, None, None]
    lane_token = jnp.sum(jnp.where(slot_hits, token_iota + 1, 0), axis=(0, 1)) - 1
    lane_token = jnp.where(lane_token < 0, tok_rows, lane_token)
    combine = jnp.sum(jnp.where(slot_hits, route_weight[:, :, None], 0.0), axis=1)
    tok_float = tokens.astype(jnp.float32)
    square_sum = lax.psum(jnp.sum(tok_float * tok_float, axis=1), "tp")
    full_width = columns * lax.axis_size("tp")
    normed = (tok_float * lax.rsqrt(square_sum / full_width + epsilon)[:, None]).astype(
        jnp.bfloat16
    )
    padded = jnp.concatenate([normed, jnp.zeros((1, columns), jnp.bfloat16)], axis=0)
    outgoing = padded[lane_token].reshape(experts, capacity, columns)
    arrived = lax.all_to_all(outgoing, "fs", split_axis=0, concat_axis=0, tiled=True).reshape(
        -1, columns
    )
    gate_local = gate_new[0]
    up_local = up_new[0]
    piece_rows = lax.all_gather(arrived, "tp", axis=1, tiled=True)
    gate_acc = jnp.dot(piece_rows, gate_local, preferred_element_type=jnp.float32)
    up_acc = jnp.dot(piece_rows, up_local, preferred_element_type=jnp.float32)
    hidden = (jax.nn.silu(gate_acc) * up_acc).astype(jnp.bfloat16)
    down_local = down_new[0]
    summed = lax.psum_scatter(
        lax.dot_general(
            down_local, hidden, (((1,), (1,)), ((), ())), preferred_element_type=jnp.float32
        ).astype(jnp.bfloat16),
        "tp",
        scatter_dimension=0,
        tiled=True,
    ).astype(jnp.float32)
    own_columns = summed.shape[0]
    outgoing_back = summed.astype(jnp.bfloat16).reshape(own_columns, fs_count, capacity)
    returned = lax.all_to_all(outgoing_back, "fs", split_axis=1, concat_axis=1, tiled=True).reshape(
        own_columns, experts * capacity
    )
    mixed = lax.dot_general(
        combine,
        returned.astype(jnp.float32),
        (((1,), (1,)), ((), ())),
        precision=lax.Precision.HIGHEST,
        preferred_element_type=jnp.float32,
    )
    return (mixed.astype(jnp.bfloat16), gate_new, up_new, down_new)


MESH = pl.DeviceIdType.MESH
STAGES = 2
HALVES = 2
LAG = 3
ROW_TILE = 256
ISSUE = (3, 1, 2)
ARRIVE = (1, 3, 2)


def flip(index, distance):
    bit = 1
    while bit <= distance:
        if distance & bit:
            index = index + bit - 2 * bit * ((index // bit) % 2)
        bit *= 2
    return index


def rows_of(index, size):
    return pl.ds(pl.multiple_of(index * size, size), size)


def moe_kernel(
    fs,
    tp,
    tokens,
    gain,
    gate,
    up,
    down,
    route,
    route_weight,
    mixed,
    w_gate,
    w_up,
    w_down,
    gain_row,
    routes,
    weights_of,
    loaded,
    staged,
    tok,
    gated,
    up_acc,
    hidden,
    pair_own,
    pair_out,
    pair_in,
    chain_in,
    chain_out,
    back_in,
    share,
    mix_out,
    mix_in,
    gain_col,
    load_sem,
    small_sem,
    tf_s,
    tf_r,
    az_s,
    az_r,
    as_s,
    as_r,
    w_s,
    g_r,
    u_r,
    dn_r,
    pr_s,
    pr_r,
    ch_s,
    ch_r,
    bk_s,
    bk_r,
    mx_s,
    mx_r,
):
    chips = tp // 2
    last = chips - 1
    f = lax.axis_index("fs")
    t = lax.axis_index("tp")
    z, core = t // 2, t % 2
    sibling = flip(t, 1)
    onward = t + 4 * core - 2
    place = core * z + (1 - core) * (last - z)
    block, width = tokens.shape
    depth, units = gate.shape[1], gate.shape[2]
    sub = width // STAGES
    half = fs * block // HALVES
    sources, finals = (gate, up, down), (w_gate, w_up, w_down)

    barrier = pltpu.get_barrier_semaphore()
    for d in range(1, fs):
        pl.semaphore_signal(barrier, inc=1, device_id={"fs": flip(f, d)}, device_id_type=MESH)
    near = [1] + list(range(2, tp, 2))
    for d in near:
        pl.semaphore_signal(barrier, inc=1, device_id={"tp": flip(t, d)}, device_id_type=MESH)

    def tok_at(k, d):
        return tok.at[k, rows_of(flip(f, d), block)]

    small = [
        pltpu.make_async_copy(source, target, small_sem.at[n])
        for n, (source, target) in enumerate(
            (
                (tokens, tok_at(t, 0)),
                (gain, gain_row),
                (route, routes),
                (route_weight, weights_of),
            )
        )
    ]
    for copy in small:
        copy.start()
    loads = {}

    def load(p, d):
        loads[p, d] = pltpu.make_async_copy(
            sources[p].at[flip(f, d)], loaded.at[p, d], load_sem.at[p, d]
        )
        loads[p, d].start()

    for d in ISSUE:
        load(0, d)
    for copy in small:
        copy.wait()
    pl.semaphore_wait(barrier, fs - 1 + len(near))

    def remote(src, dst, s_sem, r_sem, **device):
        return pltpu.make_async_remote_copy(
            src_ref=src,
            dst_ref=dst,
            send_sem=s_sem,
            recv_sem=r_sem,
            device_id=device,
            device_id_type=MESH,
        )

    def send(*args, **device):
        copy = remote(*args, **device)
        copy.start()
        return copy

    def send_if(condition, *args, **device):
        @pl.when(condition)
        def _():
            remote(*args, **device).start()

    def take(ref, sem):
        pltpu.make_async_copy(ref, ref, sem).wait()

    tok_fs = {
        d: send(tok_at(t, 0), tok_at(t, 0), tf_s, tf_r.at[d], fs=flip(f, d)) for d in ISSUE
    }

    def spread(d):
        piece = tok_at(t, d)
        send_if(z < last, piece, piece, az_s.at[0], az_r.at[z, d], tp=t + 2)
        send_if(z > 0, piece, piece, az_s.at[1], az_r.at[z, d], tp=t - 2)
        send(piece, piece, as_s, as_r, tp=sibling)

    def relay(step, d):
        for way in range(2):
            towards = 1 - 2 * way
            here = (z >= step) if way == 0 else (z + step <= last)
            more = (z < last) if way == 0 else (z > 0)
            k = t - 2 * step * towards
            origin = z - step * towards
            piece = tok_at(k, d)

            @pl.when(here)
            def _():
                take(piece, az_r.at[origin, d])

            send_if(
                jnp.logical_and(here, more),
                piece,
                piece,
                az_s.at[way],
                az_r.at[origin, d],
                tp=t + 2 * towards,
            )
            send_if(here, piece, piece, as_s, as_r, tp=sibling)

    def cast(p, d):
        loads[p, d].wait()
        tile = 64

        @pl.loop(0, depth // tile)
        def _(i):
            rows = rows_of(i, tile)
            value = loaded[p, d, rows, :]
            if p < 2:
                value = value * gain_col[rows, 0:1]
            value = value.astype(jnp.bfloat16)
            if d:
                staged[p, d - 1, rows, :] = value
            else:
                finals[p][pl.ds(pl.multiple_of(f * depth + i * tile, tile), tile), :] = value

    arrive = {}

    def ship(p, d):
        cast(p, d)
        arrive[p, d] = send(
            staged.at[p, d - 1],
            finals[p].at[rows_of(f, depth)],
            w_s,
            u_r.at[d] if p else g_r,
            fs=flip(f, d),
        )

    spread(0)
    gain_col[...] = jnp.broadcast_to(gain_row[...], (128, depth)).T
    for d in ISSUE:
        load(1, d)
    for d in ISSUE:
        ship(0, d)
    for d in ISSUE:
        load(2, d)
    for d in ISSUE:
        tok_fs[d].wait_recv()
        spread(d)
    for d in ISSUE:
        ship(1, d)
    for p in range(3):
        load(p, 0)
    for d in ISSUE:
        cast(2, d)
    for u in range(STAGES):
        for d in ISSUE:
            for c in range(2):
                arrive[2, u, d, c] = send(
                    staged.at[2, d - 1, pl.ds(c * width + u * sub, sub)],
                    w_down.at[
                        pl.ds(pl.multiple_of(f * depth + (c * width + u * sub), sub), sub)
                    ],
                    w_s,
                    dn_r.at[u, d],
                    fs=flip(f, d),
                )
    for step in range(1, chips):
        for d in (0,) + ISSUE:
            relay(step, d)
        if step == 1:
            for p in range(3):
                cast(p, 0)
            for e in range(fs):
                part = jnp.zeros((1, block), jnp.float32)
                for k in range(routes.shape[0]):
                    part = part + jnp.where(
                        routes[k : k + 1, :] == e, weights_of[k : k + 1, :], 0.0
                    )
                share[e] = jnp.broadcast_to(part, (sub, block)).T
    take(tok.at[pl.ds(0, chips)], as_r)
    take(w_gate.at[pl.ds(0, (fs - 1) * depth)], g_r)

    @pl.loop(0, fs * block // ROW_TILE)
    def _(i):
        rows = rows_of(i, ROW_TILE)
        parts = [tok[k, rows, :] for k in range(tp)]
        squares = jnp.zeros((ROW_TILE, 1), jnp.float32)
        for part in parts:
            value = part.astype(jnp.float32)
            squares = squares + jnp.sum(value * value, axis=1, keepdims=True)
        scale = lax.rsqrt(squares / (width * tp) + epsilon)
        acc = jnp.dot(
            jnp.concatenate(parts, axis=1), w_gate[...], preferred_element_type=jnp.float32
        )
        gated[rows, :] = jax.nn.silu(acc * scale) * scale

    def up_part(d, rows):
        s = flip(f, d)
        value = jnp.concatenate([tok[2 * s, rows, :], tok[2 * s + 1, rows, :]], axis=1)
        return jnp.dot(value, w_up[rows_of(s, depth), :], preferred_element_type=jnp.float32)

    early = (0,) + ARRIVE[:-1]
    for n, d in enumerate(early):
        if d:
            arrive[1, d].wait_recv()

        @pl.loop(0, fs * block // ROW_TILE)
        def _(i):
            rows = rows_of(i, ROW_TILE)
            part = up_part(d, rows)
            up_acc[rows, :] = up_acc[rows, :] + part if n else part

    arrive[1, ARRIVE[-1]].wait_recv()

    def finish_hidden(h):
        @pl.loop(0, half // ROW_TILE)
        def _(i):
            rows = pl.ds(pl.multiple_of(h * half + i * ROW_TILE, ROW_TILE), ROW_TILE)
            value = up_acc[rows, :] + up_part(ARRIVE[-1], rows)
            hidden[rows, :] = (gated[rows, :] * value).astype(jnp.bfloat16)

    pieces = [(u, 0, h) for h in range(HALVES) for u in range(STAGES)]
    pieces += [(u, d, h) for u in range(STAGES) for d in ARRIVE for h in range(HALVES)]
    count = len(pieces)

    def product(q):
        u, d, h = pieces[q]
        s = flip(f, d)
        if d == 0 and u == 0:
            finish_hidden(h)
        if d and h == 0:
            take(w_down.at[pl.ds(0, 2 * sub)], dn_r.at[u, d])

        def weights(c):
            start = pl.multiple_of(s * depth + c * width + u * sub, sub)
            return w_down[pl.ds(start, sub), :]

        @pl.loop(0, half // ROW_TILE)
        def _(i):
            rows = rows_of(i, ROW_TILE)
            value = hidden[pl.ds(pl.multiple_of(h * half + i * ROW_TILE, ROW_TILE), ROW_TILE), :]
            result = lax.dot_general(
                value,
                jnp.concatenate([weights(core), weights(1 - core)], axis=0),
                (((1,), (1,)), ((), ())),
                preferred_element_type=jnp.float32,
            )
            pair_own[q, rows, :] = result[:, :sub]
            pair_out[q, rows, :] = result[:, sub:].astype(jnp.bfloat16)

        send(pair_out.at[q], pair_in.at[q], pr_s, pr_r.at[q], tp=sibling)

    per_half = half // block

    def advance(p, j):
        u, d, h = pieces[j]
        s = flip(f, d)
        take(pair_in.at[j], pr_r.at[j])
        if p:
            take(chain_in.at[j], ch_r.at[j])

        @pl.loop(0, half // ROW_TILE)
        def _(i):
            rows = rows_of(i, ROW_TILE)
            value = pair_own[j, rows, :] + pair_in[j, rows, :].astype(jnp.float32)
            if p:
                value = value + chain_in[j, rows, :].astype(jnp.float32)
            chain_out[j, rows, :] = value.astype(jnp.bfloat16)

        if p < last:
            send(chain_out.at[j], chain_in.at[j], ch_s, ch_r.at[j], tp=onward)
            return
        for n in range(per_half):
            b = h * per_half + n
            rows = pl.ds(n * block, block)

            @pl.when(f != b)
            def _():
                send(chain_out.at[j, rows], back_in.at[u, s, f], bk_s, bk_r.at[u], fs=b)

            @pl.when(f == b)
            def _():
                back_in[u, s, f] = chain_out[j, rows, :]

    def combine(u):
        take(back_in.at[u, :, pl.ds(0, fs - 1)], bk_r.at[u])
        for s in range(fs):
            value = jnp.zeros((block, sub), jnp.float32)
            for e in range(fs):
                value = value + share[e] * back_in[u, s, e].astype(jnp.float32)
            value = value.astype(jnp.bfloat16)

            @pl.when(s == z)
            def _():
                mix_in[u] = value

            @pl.when(s != z)
            def _():
                mix_out[u, s] = value
                send(mix_out.at[u, s], mix_in.at[u], mx_s, mx_r.at[u], tp=2 * s + core)

    ready = {}
    for u in range(STAGES):
        done = max(j for j in range(count) if pieces[j][0] == u) + 1 + LAG * last
        ready[min(done + 1, count + LAG * last)] = ready.get(
            min(done + 1, count + LAG * last), []
        ) + [u]
    for q in range(count + 1 + LAG * last):
        if q < count:
            product(q)
        for p in range(chips):
            j = q - 1 - LAG * p
            if 0 <= j < count:

                @pl.when(place == p)
                def _():
                    advance(p, j)

        for u in ready.get(q, []):

            @pl.when(place == last)
            def _():
                combine(u)

    @pl.when(place < last)
    def _():
        for u in range(STAGES):
            take(mix_in.at[u], mx_r.at[u])

    for u in range(STAGES):
        mixed[:, u * sub : (u + 1) * sub] = mix_in[u]

    take(tok.at[0, pl.ds(0, (fs - 1) * block)], tf_s)
    for n in range(chips):

        @pl.when(z == n)
        def _():
            if n < last:
                take(tok.at[pl.ds(0, 1 + n)], az_s.at[0])
            if n:
                take(tok.at[pl.ds(0, chips - n)], az_s.at[1])

    take(tok.at[pl.ds(0, chips)], as_s)
    take(staged, w_s)
    take(pair_out, pr_s)

    @pl.when(place < last)
    def _():
        take(chain_out, ch_s)

    @pl.when(place == last)
    def _():
        take(back_in.at[:, :, pl.ds(0, fs - 1)], bk_s)
        take(mix_out.at[:, pl.ds(0, chips - 1)], mx_s)


def write_kernel(*refs):
    sem = refs[-1]
    count = len(refs) // 2
    copies = [
        pltpu.make_async_copy(refs[i], refs[count + i].at[0] if i else refs[count], sem.at[i])
        for i in range(count)
    ]
    for copy in copies:
        copy.start()
    for copy in copies:
        copy.wait()


def write_out(mixed, *weights):
    whole = pl.BlockSpec(memory_space=pltpu.VMEM)
    far = pl.BlockSpec(memory_space=pl.ANY)
    shapes = [jax.ShapeDtypeStruct(mixed.shape, mixed.dtype)]
    shapes += [jax.ShapeDtypeStruct((1,) + w.shape, w.dtype) for w in weights]
    return pl.pallas_call(
        write_kernel,
        out_shape=tuple(shapes),
        in_specs=[whole] * len(shapes),
        out_specs=tuple([far] * len(shapes)),
        scratch_shapes=[pltpu.SemaphoreType.DMA((len(shapes),))],
        compiler_params=pltpu.CompilerParams(vmem_limit_bytes=1024 * 1024),
    )(mixed, *weights)


def dense_body(tokens, norm_gain, gate_weight, up_weight, down_weight, route, route_weight):
    fs, tp = lax.axis_size("fs"), lax.axis_size("tp")
    block, width = tokens.shape
    experts, depth, units = gate_weight.shape
    rows, full, sub, chips = fs * block, tp * width, width // STAGES, tp // 2
    count, half = STAGES * fs * HALVES, rows // HALVES
    whole = pl.BlockSpec(memory_space=pltpu.VMEM)
    far = pl.BlockSpec(memory_space=pl.ANY)
    narrow, wide, dma = jnp.bfloat16, jnp.float32, pltpu.SemaphoreType.DMA
    weight = pltpu.VMEM((full, units), narrow)
    mixed, gate_new, up_new, down_new = pl.pallas_call(
        functools.partial(moe_kernel, fs, tp),
        out_shape=(pltpu.VMEM((block, width), narrow), weight, weight, weight),
        in_specs=[far] * 7,
        out_specs=(whole, whole, whole, whole),
        scratch_shapes=[
            pltpu.VMEM((1, depth), wide),
            pltpu.VMEM((route.shape[1], block), jnp.int32),
            pltpu.VMEM((route.shape[1], block), wide),
            pltpu.VMEM((3, experts, depth, units), wide),
            pltpu.VMEM((3, fs - 1, depth, units), narrow),
            pltpu.VMEM((tp, rows, width), narrow),
            pltpu.VMEM((rows, units), wide),
            pltpu.VMEM((rows, units), wide),
            pltpu.VMEM((rows, units), narrow),
            pltpu.VMEM((count, half, sub), wide),
            pltpu.VMEM((count, half, sub), narrow),
            pltpu.VMEM((count, half, sub), narrow),
            pltpu.VMEM((count, half, sub), narrow),
            pltpu.VMEM((count, half, sub), narrow),
            pltpu.VMEM((STAGES, fs, fs, block, sub), narrow),
            pltpu.VMEM((fs, block, sub), wide),
            pltpu.VMEM((STAGES, fs, block, sub), narrow),
            pltpu.VMEM((STAGES, block, sub), narrow),
            pltpu.VMEM((depth, 128), wide),
            dma((3, experts)),
            dma((4,)),
            dma,
            dma((fs,)),
            dma((2,)),
            dma((chips, fs)),
            dma,
            dma,
            dma,
            dma,
            dma((fs,)),
            dma((STAGES, fs)),
            dma,
            dma((count,)),
            dma,
            dma((count,)),
            dma,
            dma((STAGES,)),
            dma,
            dma((STAGES,)),
        ],
        compiler_params=pltpu.CompilerParams(
            collective_id=0, has_side_effects=True, vmem_limit_bytes=56 * 1024 * 1024
        ),
    )(tokens, norm_gain[None, :], gate_weight, up_weight, down_weight, route.T, route_weight.T)
    return write_out(mixed, gate_new, up_new, down_new)


def body(tokens, norm_gain, gate_weight, up_weight, down_weight, route, route_weight):
    fs, tp = lax.axis_size("fs"), lax.axis_size("tp")
    fits = (
        fs == 4
        and tp == 2 * fs
        and gate_weight.shape[0] == fs
        and tokens.shape[1] % (128 * STAGES) == 0
        and tokens.shape[0] % ROW_TILE == 0
        and gate_weight.shape[1] == 2 * tokens.shape[1]
        and tokens.shape[0] * fs * tokens.shape[1] * tp <= 1024 * 2048
    )
    chosen = dense_body if fits else slotted_body
    return chosen(tokens, norm_gain, gate_weight, up_weight, down_weight, route, route_weight)


def solution(mesh):
    in_specs = (
        P("fs", "tp"),
        P("fs"),
        P(None, "fs", "tp"),
        P(None, "fs", "tp"),
        P(None, "fs", "tp"),
        P("fs", None),
        P("fs", None),
    )
    out_specs = (P("fs", "tp"), P("fs", None, "tp"), P("fs", None, "tp"), P("fs", None, "tp"))
    return jax.shard_map(body, mesh=mesh, in_specs=in_specs, out_specs=out_specs, check_vma=False)
```

```python
import functools

import jax
import jax.numpy as jnp
from jax import lax
from jax.experimental import pallas as pl
from jax.experimental.pallas import tpu as pltpu
from jax.sharding import PartitionSpec as P

epsilon = 1e-05


def slot_table(route, block_rows, expert_count):
    pair_ids = route.reshape(-1, block_rows * route.shape[1])
    onehot = (
        pair_ids[:, :, None] == jnp.arange(expert_count, dtype=jnp.int32)[None, None, :]
    ).astype(jnp.int32)
    before = jnp.cumsum(onehot, axis=1) - onehot
    return jnp.sum(before * onehot, axis=2).reshape(route.shape)


def slotted_body(tokens, norm_gain, gate_weight, up_weight, down_weight, route, route_weight):
    experts = gate_weight.shape[0]
    tok_rows = tokens.shape[0]
    columns = tokens.shape[1]
    fs_count = lax.axis_size("fs")
    capacity = 4 * tok_rows // fs_count
    gain_col = norm_gain[None, :, None]
    gate_cast = (gate_weight * gain_col).astype(jnp.bfloat16)
    up_cast = (up_weight * gain_col).astype(jnp.bfloat16)
    down_cast = down_weight.astype(jnp.bfloat16)
    gate_new, up_new, down_new = (
        lax.all_to_all(gate_cast, "fs", split_axis=0, concat_axis=1, tiled=True),
        lax.all_to_all(up_cast, "fs", split_axis=0, concat_axis=1, tiled=True),
        lax.all_to_all(down_cast, "fs", split_axis=0, concat_axis=1, tiled=True),
    )
    slot_of = slot_table(route, tok_rows, experts)
    target = route * capacity + slot_of
    slot_lanes = jnp.arange(experts * capacity, dtype=jnp.int32)
    slot_hits = target[:, :, None] == slot_lanes[None, None, :]
    token_iota = jnp.arange(tok_rows, dtype=jnp.int32)[:, None, None]
    lane_token = jnp.sum(jnp.where(slot_hits, token_iota + 1, 0), axis=(0, 1)) - 1
    lane_token = jnp.where(lane_token < 0, tok_rows, lane_token)
    combine = jnp.sum(jnp.where(slot_hits, route_weight[:, :, None], 0.0), axis=1)
    tok_float = tokens.astype(jnp.float32)
    square_sum = lax.psum(jnp.sum(tok_float * tok_float, axis=1), "tp")
    full_width = columns * lax.axis_size("tp")
    normed = (tok_float * lax.rsqrt(square_sum / full_width + epsilon)[:, None]).astype(
        jnp.bfloat16
    )
    padded = jnp.concatenate([normed, jnp.zeros((1, columns), jnp.bfloat16)], axis=0)
    outgoing = padded[lane_token].reshape(experts, capacity, columns)
    arrived = lax.all_to_all(outgoing, "fs", split_axis=0, concat_axis=0, tiled=True).reshape(
        -1, columns
    )
    gate_local = gate_new[0]
    up_local = up_new[0]
    piece_rows = lax.all_gather(arrived, "tp", axis=1, tiled=True)
    gate_acc = jnp.dot(piece_rows, gate_local, preferred_element_type=jnp.float32)
    up_acc = jnp.dot(piece_rows, up_local, preferred_element_type=jnp.float32)
    hidden = (jax.nn.silu(gate_acc) * up_acc).astype(jnp.bfloat16)
    down_local = down_new[0]
    summed = lax.psum_scatter(
        lax.dot_general(
            down_local, hidden, (((1,), (1,)), ((), ())), preferred_element_type=jnp.float32
        ).astype(jnp.bfloat16),
        "tp",
        scatter_dimension=0,
        tiled=True,
    ).astype(jnp.float32)
    own_columns = summed.shape[0]
    outgoing_back = summed.astype(jnp.bfloat16).reshape(own_columns, fs_count, capacity)
    returned = lax.all_to_all(outgoing_back, "fs", split_axis=1, concat_axis=1, tiled=True).reshape(
        own_columns, experts * capacity
    )
    mixed = lax.dot_general(
        combine,
        returned.astype(jnp.float32),
        (((1,), (1,)), ((), ())),
        precision=lax.Precision.HIGHEST,
        preferred_element_type=jnp.float32,
    )
    return (mixed.astype(jnp.bfloat16), gate_new, up_new, down_new)


MESH = pl.DeviceIdType.MESH
STAGES = 2
QUARTERS = 4
ISSUE = (1, 2, 3)
EXPECTED = (7.0, 13.0, 16.0, 20.0, 22.0, 24.0, 28.0, 30.0, 32.0)
RETURN = 4


def flip(index, distance):
    bit = 1
    while bit <= distance:
        if distance & bit:
            index = index + bit - 2 * bit * ((index // bit) % 2)
        bit *= 2
    return index


def plan(works, pieces, chips):
    hop, pair, cost = 4.7, 2.0, 0.5
    starts, needs, now = [], [{}, {}], 0.0
    for w, (j, at, sides) in enumerate(works):
        now = max(now, at)
        starts.append(now)
        now = now + cost
        for side in sides:
            needs[side][j] = (w, now)
    steps = [[[] for _ in range(chips)] for _ in works]
    before = [0.0] * pieces
    for p in range(chips):
        side, leave, floor = 2 * p // chips, 0.0, 0
        for j in range(pieces):
            w, done = needs[side][j]
            there = max(done + pair, before[j] + hop if p else 0.0)
            floor = max([floor, w] + [i for i, begin in enumerate(starts) if begin <= there])
            steps[floor][p].append(j)
            leave = max(leave + 1.0, there)
            before[j] = leave
    return steps


def rows_of(index, size):
    return pl.ds(pl.multiple_of(index * size, size), size)


def moe_kernel(
    fs,
    tp,
    tokens,
    gain,
    gate,
    up,
    down,
    route,
    route_weight,
    mixed,
    w_gate,
    w_up,
    w_down,
    gain_row,
    routes,
    weights_of,
    loaded,
    staged,
    tok,
    gated,
    up_acc,
    hidden,
    pair_own,
    pair_out,
    pair_in,
    chain_in,
    chain_out,
    back_in,
    share,
    mix_out,
    mix_in,
    gain_col,
    load_sem,
    small_sem,
    tf_s,
    tf_r,
    az_s,
    az_r,
    as_s,
    as_r,
    w_s,
    g_r,
    u_r,
    dn_r,
    pr_s,
    pr_r,
    ch_s,
    ch_r,
    bk_s,
    bk_r,
    mx_s,
    mx_r,
):
    chips = tp // 2
    last = chips - 1
    f = lax.axis_index("fs")
    t = lax.axis_index("tp")
    z, core = t // 2, t % 2
    sibling = flip(t, 1)
    onward = t + 4 * core - 2
    place = core * z + (1 - core) * (last - z)
    strip, width = tokens.shape[1], tokens.shape[2]
    depth, units = gate.shape[1], gate.shape[2]
    block, rows_all = QUARTERS * strip, fs * QUARTERS * strip
    sub = width // STAGES
    piece_rows = fs * strip
    first = 1 - z // (chips // 2)
    sources, finals = (gate, up, down), (w_gate, w_up, w_down)

    barrier = pltpu.get_barrier_semaphore()
    for d in range(1, fs):
        pl.semaphore_signal(barrier, inc=1, device_id={"fs": flip(f, d)}, device_id_type=MESH)
    near = [1] + list(range(2, tp, 2))
    for d in near:
        pl.semaphore_signal(barrier, inc=1, device_id={"tp": flip(t, d)}, device_id_type=MESH)

    def tok_at(k, d):
        return tok.at[k, :, flip(f, d)]

    small = [
        pltpu.make_async_copy(source, target, small_sem.at[n])
        for n, (source, target) in enumerate(
            (
                (tokens, tok_at(t, 0)),
                (gain, gain_row),
                (route, routes),
                (route_weight, weights_of),
            )
        )
    ]
    for copy in small:
        copy.start()
    loads = {}

    def load(p, d):
        loads[p, d] = pltpu.make_async_copy(
            sources[p].at[flip(f, d)], loaded.at[p, d], load_sem.at[p, d]
        )
        loads[p, d].start()

    for d in ISSUE:
        load(0, d)
    for copy in small:
        copy.wait()
    pl.semaphore_wait(barrier, fs - 1 + len(near))

    def remote(src, dst, s_sem, r_sem, **device):
        return pltpu.make_async_remote_copy(
            src_ref=src,
            dst_ref=dst,
            send_sem=s_sem,
            recv_sem=r_sem,
            device_id=device,
            device_id_type=MESH,
        )

    def send(*args, **device):
        copy = remote(*args, **device)
        copy.start()
        return copy

    def send_if(condition, *args, **device):
        @pl.when(condition)
        def _():
            remote(*args, **device).start()

    def take(ref, sem):
        pltpu.make_async_copy(ref, ref, sem).wait()

    tok_fs = {
        d: send(tok_at(t, 0), tok_at(t, 0), tf_s, tf_r.at[d], fs=flip(f, d)) for d in ISSUE
    }

    def spread(d):
        piece = tok_at(t, d)
        send_if(z < last, piece, piece, az_s.at[0], az_r.at[z, d], tp=t + 2)
        send_if(z > 0, piece, piece, az_s.at[1], az_r.at[z, d], tp=t - 2)
        send(piece, piece, as_s, as_r, tp=sibling)

    def relay(step, d):
        for way in range(2):
            towards = 1 - 2 * way
            here = (z >= step) if way == 0 else (z + step <= last)
            more = (z < last) if way == 0 else (z > 0)
            k = t - 2 * step * towards
            origin = z - step * towards
            piece = tok_at(k, d)

            @pl.when(here)
            def _():
                take(piece, az_r.at[origin, d])

            send_if(
                jnp.logical_and(here, more),
                piece,
                piece,
                az_s.at[way],
                az_r.at[origin, d],
                tp=t + 2 * towards,
            )
            send_if(here, piece, piece, as_s, as_r, tp=sibling)

    def cast(p, d):
        loads[p, d].wait()
        tile = 64

        @pl.loop(0, depth // tile)
        def _(i):
            rows = rows_of(i, tile)
            value = loaded[p, d, rows, :]
            if p < 2:
                value = value * gain_col[rows, 0:1]
            value = value.astype(jnp.bfloat16)
            if d:
                staged[p, d - 1, rows, :] = value
            else:
                finals[p][pl.ds(pl.multiple_of(f * depth + i * tile, tile), tile), :] = value

    arrive = {}

    def ship(p, d):
        cast(p, d)
        arrive[p, d] = send(
            staged.at[p, d - 1],
            finals[p].at[rows_of(f, depth)],
            w_s,
            u_r.at[d] if p else g_r,
            fs=flip(f, d),
        )

    spread(0)
    gain_col[...] = jnp.broadcast_to(gain_row[...], (128, depth)).T
    for d in ISSUE:
        load(1, d)
    for d in ISSUE:
        ship(0, d)
    for d in ISSUE:
        load(2, d)
    for d in ISSUE:
        tok_fs[d].wait_recv()
        spread(d)
    for d in ISSUE:
        ship(1, d)
    for p in range(3):
        load(p, 0)
    for d in ISSUE:
        cast(2, d)
    def send_down(u, d, c, r_sem):
        send(
            staged.at[2, d - 1, pl.ds(pl.multiple_of(c * width + u * sub, sub), sub)],
            w_down.at[pl.ds(pl.multiple_of(f * depth + c * width + u * sub, sub), sub)],
            w_s,
            r_sem,
            fs=flip(f, d),
        )

    for u in range(STAGES - 1):
        for d in ISSUE:
            for c in range(2):
                send_down(u, d, c, dn_r.at[u, d])
    for side in range(2):
        for d in ISSUE:
            c = 1 - first if side else first
            send_down(STAGES - 1, d, c, dn_r.at[STAGES - 1 + side, d])
    for step in range(1, chips):
        for d in (0,) + ISSUE:
            relay(step, d)
        if step == 1:
            for p in range(3):
                cast(p, 0)
            for e in range(fs):
                part = jnp.zeros((1, block), jnp.float32)
                for k in range(routes.shape[0]):
                    part = part + jnp.where(
                        routes[k : k + 1, :] == e, weights_of[k : k + 1, :], 0.0
                    )
                share[e] = jnp.broadcast_to(part, (sub, block)).T
    take(tok.at[pl.ds(0, chips)], as_r)
    take(w_gate.at[pl.ds(0, (fs - 1) * depth)], g_r)

    def tok_rows(k, i):
        return tok[k, i].reshape(piece_rows, width)

    @pl.loop(0, QUARTERS)
    def _(i):
        rows = rows_of(i, piece_rows)
        parts = [tok_rows(k, i) for k in range(tp)]
        squares = jnp.zeros((piece_rows, 1), jnp.float32)
        for part in parts:
            value = part.astype(jnp.float32)
            squares = squares + jnp.sum(value * value, axis=1, keepdims=True)
        scale = lax.rsqrt(squares / (width * tp) + epsilon)
        acc = jnp.dot(
            jnp.concatenate(parts, axis=1), w_gate[...], preferred_element_type=jnp.float32
        )
        gated[rows, :] = jax.nn.silu(acc * scale) * scale

    def up_part(d, i):
        s = flip(f, d)
        value = jnp.concatenate([tok_rows(2 * s, i), tok_rows(2 * s + 1, i)], axis=1)
        return jnp.dot(value, w_up[rows_of(s, depth), :], preferred_element_type=jnp.float32)

    early = (0,) + ISSUE[:-1]
    for n, d in enumerate(early):
        if d:
            arrive[1, d].wait_recv()

        @pl.loop(0, QUARTERS)
        def _(i):
            rows = rows_of(i, piece_rows)
            part = up_part(d, i)
            up_acc[rows, :] = up_acc[rows, :] + part if n else part

    arrive[1, ISSUE[-1]].wait_recv()

    def finish_hidden(h):
        rows = pl.ds(h * piece_rows, piece_rows)
        value = up_acc[rows, :] + up_part(ISSUE[-1], h)
        hidden[rows, :] = (gated[rows, :] * value).astype(jnp.bfloat16)

    end = STAGES - 1
    pieces = [(u, 0, h) for h in range(QUARTERS) for u in range(STAGES)]
    pieces += [(u, d, h) for u in range(STAGES) for d in ISSUE for h in range(QUARTERS)]
    count = len(pieces)

    def product(j, side):
        u, d, h = pieces[j]
        s = flip(f, d)
        if d == 0 and u == 0:
            finish_hidden(h)
        if d and h == 0:
            size = 2 * sub if side is None else sub
            take(w_down.at[pl.ds(0, size)], dn_r.at[u + (side or 0), d])

        def weights(c):
            start = pl.multiple_of(s * depth + c * width + u * sub, sub)
            return w_down[pl.ds(start, sub), :]

        def times(weight):
            return lax.dot_general(
                hidden[pl.ds(h * piece_rows, piece_rows), :],
                weight,
                (((1,), (1,)), ((), ())),
                preferred_element_type=jnp.float32,
            )

        def give(value):
            pair_out[j] = value.astype(jnp.bfloat16)
            send(pair_out.at[j], pair_in.at[j], pr_s, pr_r.at[j], tp=sibling)

        if side is None:
            result = times(jnp.concatenate([weights(core), weights(1 - core)], axis=0))
            pair_own[j] = result[:, :sub]
            give(result[:, sub:])
            return
        c = 1 - first if side else first
        result = times(weights(c))

        @pl.when(core == c)
        def _():
            pair_own[j] = result

        @pl.when(core != c)
        def _():
            give(result)

    def advance(p, j):
        u, d, h = pieces[j]
        s = flip(f, d)
        take(pair_in.at[j], pr_r.at[j])
        if p:
            take(chain_in.at[j], ch_r.at[j])

        value = pair_own[j] + pair_in[j].astype(jnp.float32)
        if p:
            value = value + chain_in[j].astype(jnp.float32)
        chain_out[j] = value.astype(jnp.bfloat16)

        if p < last:
            send(chain_out.at[j], chain_in.at[j], ch_s, ch_r.at[j], tp=onward)
            return
        for b in range(fs):
            rows = pl.ds(b * strip, strip)

            @pl.when(f != b)
            def _():
                send(chain_out.at[j, rows], back_in.at[u, h, s, f], bk_s, bk_r.at[u, h], fs=b)

            @pl.when(f == b)
            def _():
                back_in[u, h, s, f] = chain_out[j, rows, :]

    def combine(u, h):
        take(back_in.at[u, h, :, pl.ds(0, fs - 1)], bk_r.at[u, h])
        for s in range(fs):
            value = jnp.zeros((strip, sub), jnp.float32)
            for e in range(fs):
                value = value + share[e, pl.ds(h * strip, strip), :] * back_in[u, h, s, e].astype(
                    jnp.float32
                )
            value = value.astype(jnp.bfloat16)

            @pl.when(s == z)
            def _():
                mix_in[u, h] = value

            @pl.when(s != z)
            def _():
                mix_out[u, h, s] = value
                send(mix_out.at[u, h, s], mix_in.at[u, h], mx_s, mx_r.at[u, h], tp=2 * s + core)

    works = [(j, 0.0, (0, 1)) for j in range(STAGES * QUARTERS)]
    times_of = iter(EXPECTED)
    index = {piece: j for j, piece in enumerate(pieces)}
    for u in range(STAGES):
        for side in (0, 1) if u == end else (None,):
            for d in ISSUE:
                at = next(times_of)
                sides = (0, 1) if side is None else (side,)
                works += [(index[u, d, h], at, sides) for h in range(QUARTERS)]
    steps = plan(works, count, chips)
    split = {j for j in range(count) if pieces[j][0] == end and pieces[j][1]}
    waiting = [(u, h) for u in range(STAGES) for h in range(QUARTERS)]
    for w, (j, _, sides) in enumerate(works):
        product(j, sides[0] if j in split else None)
        for p in range(chips):
            if not steps[w][p]:
                continue

            @pl.when(place == p)
            def _():
                for i in steps[w][p]:
                    advance(p, i)
                    if p == last and waiting[0][0] < end and i >= count - len(split) + RETURN:
                        combine(*waiting.pop(0))

    @pl.when(place == last)
    def _():
        for u, h in waiting:
            combine(u, h)

    @pl.when(place < last)
    def _():
        for u in range(STAGES):
            for h in range(QUARTERS):
                take(mix_in.at[u, h], mx_r.at[u, h])

    for u in range(STAGES):
        mixed[:, u * sub : (u + 1) * sub] = mix_in[u].reshape(block, sub)

    take(tok.at[0, :, pl.ds(0, fs - 1)], tf_s)
    for n in range(chips):

        @pl.when(z == n)
        def _():
            if n < last:
                take(tok.at[pl.ds(0, 1 + n)], az_s.at[0])
            if n:
                take(tok.at[pl.ds(0, chips - n)], az_s.at[1])

    take(tok.at[pl.ds(0, chips)], as_s)
    take(staged, w_s)
    take(pair_out, pr_s)

    @pl.when(place < last)
    def _():
        take(chain_out, ch_s)

    @pl.when(place == last)
    def _():
        take(back_in.at[:, :, :, pl.ds(0, fs - 1)], bk_s)
        take(mix_out.at[:, :, pl.ds(0, chips - 1)], mx_s)


def write_kernel(*refs):
    sem = refs[-1]
    count = len(refs) // 2
    copies = [
        pltpu.make_async_copy(refs[i], refs[count + i].at[0] if i else refs[count], sem.at[i])
        for i in range(count)
    ]
    for copy in copies:
        copy.start()
    for copy in copies:
        copy.wait()


def write_out(mixed, *weights):
    whole = pl.BlockSpec(memory_space=pltpu.VMEM)
    far = pl.BlockSpec(memory_space=pl.ANY)
    shapes = [jax.ShapeDtypeStruct(mixed.shape, mixed.dtype)]
    shapes += [jax.ShapeDtypeStruct((1,) + w.shape, w.dtype) for w in weights]
    return pl.pallas_call(
        write_kernel,
        out_shape=tuple(shapes),
        in_specs=[whole] * len(shapes),
        out_specs=tuple([far] * len(shapes)),
        scratch_shapes=[pltpu.SemaphoreType.DMA((len(shapes),))],
        compiler_params=pltpu.CompilerParams(vmem_limit_bytes=1024 * 1024),
    )(mixed, *weights)


def dense_body(tokens, norm_gain, gate_weight, up_weight, down_weight, route, route_weight):
    fs, tp = lax.axis_size("fs"), lax.axis_size("tp")
    block, width = tokens.shape
    experts, depth, units = gate_weight.shape
    rows, full, sub, chips = fs * block, tp * width, width // STAGES, tp // 2
    count, strip = STAGES * fs * QUARTERS, block // QUARTERS
    piece = fs * strip
    whole = pl.BlockSpec(memory_space=pltpu.VMEM)
    far = pl.BlockSpec(memory_space=pl.ANY)
    narrow, wide, dma = jnp.bfloat16, jnp.float32, pltpu.SemaphoreType.DMA
    weight = pltpu.VMEM((full, units), narrow)
    mixed, gate_new, up_new, down_new = pl.pallas_call(
        functools.partial(moe_kernel, fs, tp),
        out_shape=(pltpu.VMEM((block, width), narrow), weight, weight, weight),
        in_specs=[far] * 7,
        out_specs=(whole, whole, whole, whole),
        scratch_shapes=[
            pltpu.VMEM((1, depth), wide),
            pltpu.VMEM((route.shape[1], block), jnp.int32),
            pltpu.VMEM((route.shape[1], block), wide),
            pltpu.VMEM((3, experts, depth, units), wide),
            pltpu.VMEM((3, fs - 1, depth, units), narrow),
            pltpu.VMEM((tp, QUARTERS, fs, strip, width), narrow),
            pltpu.VMEM((rows, units), wide),
            pltpu.VMEM((rows, units), wide),
            pltpu.VMEM((rows, units), narrow),
            pltpu.VMEM((count, piece, sub), wide),
            pltpu.VMEM((count, piece, sub), narrow),
            pltpu.VMEM((count, piece, sub), narrow),
            pltpu.VMEM((count, piece, sub), narrow),
            pltpu.VMEM((count, piece, sub), narrow),
            pltpu.VMEM((STAGES, QUARTERS, fs, fs, strip, sub), narrow),
            pltpu.VMEM((fs, block, sub), wide),
            pltpu.VMEM((STAGES, QUARTERS, fs, strip, sub), narrow),
            pltpu.VMEM((STAGES, QUARTERS, strip, sub), narrow),
            pltpu.VMEM((depth, 128), wide),
            dma((3, experts)),
            dma((4,)),
            dma,
            dma((fs,)),
            dma((2,)),
            dma((chips, fs)),
            dma,
            dma,
            dma,
            dma,
            dma((fs,)),
            dma((STAGES + 1, fs)),
            dma,
            dma((count,)),
            dma,
            dma((count,)),
            dma,
            dma((STAGES, QUARTERS)),
            dma,
            dma((STAGES, QUARTERS)),
        ],
        compiler_params=pltpu.CompilerParams(
            collective_id=0, has_side_effects=True, vmem_limit_bytes=56 * 1024 * 1024
        ),
    )(
        tokens.reshape(QUARTERS, strip, width),
        norm_gain[None, :],
        gate_weight,
        up_weight,
        down_weight,
        route.T,
        route_weight.T,
    )
    return write_out(mixed, gate_new, up_new, down_new)


def body(tokens, norm_gain, gate_weight, up_weight, down_weight, route, route_weight):
    fs, tp = lax.axis_size("fs"), lax.axis_size("tp")
    fits = (
        fs == 4
        and tp == 2 * fs
        and gate_weight.shape[0] == fs
        and tokens.shape[1] % (128 * STAGES) == 0
        and tokens.shape[0] % (64 * QUARTERS) == 0
        and gate_weight.shape[1] == 2 * tokens.shape[1]
        and tokens.shape[0] * fs * tokens.shape[1] * tp <= 1024 * 2048
    )
    chosen = dense_body if fits else slotted_body
    return chosen(tokens, norm_gain, gate_weight, up_weight, down_weight, route, route_weight)


def solution(mesh):
    in_specs = (
        P("fs", "tp"),
        P("fs"),
        P(None, "fs", "tp"),
        P(None, "fs", "tp"),
        P(None, "fs", "tp"),
        P("fs", None),
        P("fs", None),
    )
    out_specs = (P("fs", "tp"), P("fs", None, "tp"), P("fs", None, "tp"), P("fs", None, "tp"))
    return jax.shard_map(body, mesh=mesh, in_specs=in_specs, out_specs=out_specs, check_vma=False)
```

```python
import functools

import jax
import jax.numpy as jnp
from jax import lax
from jax.experimental import pallas as pl
from jax.experimental.pallas import tpu as pltpu
from jax.sharding import PartitionSpec as P

epsilon = 1e-05


def slot_table(route, block_rows, expert_count):
    pair_ids = route.reshape(-1, block_rows * route.shape[1])
    onehot = (
        pair_ids[:, :, None] == jnp.arange(expert_count, dtype=jnp.int32)[None, None, :]
    ).astype(jnp.int32)
    before = jnp.cumsum(onehot, axis=1) - onehot
    return jnp.sum(before * onehot, axis=2).reshape(route.shape)


def slotted_body(tokens, norm_gain, gate_weight, up_weight, down_weight, route, route_weight):
    experts = gate_weight.shape[0]
    tok_rows = tokens.shape[0]
    columns = tokens.shape[1]
    fs_count = lax.axis_size("fs")
    capacity = 4 * tok_rows // fs_count
    gain_col = norm_gain[None, :, None]
    gate_cast = (gate_weight * gain_col).astype(jnp.bfloat16)
    up_cast = (up_weight * gain_col).astype(jnp.bfloat16)
    down_cast = down_weight.astype(jnp.bfloat16)
    gate_new, up_new, down_new = (
        lax.all_to_all(gate_cast, "fs", split_axis=0, concat_axis=1, tiled=True),
        lax.all_to_all(up_cast, "fs", split_axis=0, concat_axis=1, tiled=True),
        lax.all_to_all(down_cast, "fs", split_axis=0, concat_axis=1, tiled=True),
    )
    slot_of = slot_table(route, tok_rows, experts)
    target = route * capacity + slot_of
    slot_lanes = jnp.arange(experts * capacity, dtype=jnp.int32)
    slot_hits = target[:, :, None] == slot_lanes[None, None, :]
    token_iota = jnp.arange(tok_rows, dtype=jnp.int32)[:, None, None]
    lane_token = jnp.sum(jnp.where(slot_hits, token_iota + 1, 0), axis=(0, 1)) - 1
    lane_token = jnp.where(lane_token < 0, tok_rows, lane_token)
    combine = jnp.sum(jnp.where(slot_hits, route_weight[:, :, None], 0.0), axis=1)
    tok_float = tokens.astype(jnp.float32)
    square_sum = lax.psum(jnp.sum(tok_float * tok_float, axis=1), "tp")
    full_width = columns * lax.axis_size("tp")
    normed = (tok_float * lax.rsqrt(square_sum / full_width + epsilon)[:, None]).astype(
        jnp.bfloat16
    )
    padded = jnp.concatenate([normed, jnp.zeros((1, columns), jnp.bfloat16)], axis=0)
    outgoing = padded[lane_token].reshape(experts, capacity, columns)
    arrived = lax.all_to_all(outgoing, "fs", split_axis=0, concat_axis=0, tiled=True).reshape(
        -1, columns
    )
    gate_local = gate_new[0]
    up_local = up_new[0]
    piece_rows = lax.all_gather(arrived, "tp", axis=1, tiled=True)
    gate_acc = jnp.dot(piece_rows, gate_local, preferred_element_type=jnp.float32)
    up_acc = jnp.dot(piece_rows, up_local, preferred_element_type=jnp.float32)
    hidden = (jax.nn.silu(gate_acc) * up_acc).astype(jnp.bfloat16)
    down_local = down_new[0]
    summed = lax.psum_scatter(
        lax.dot_general(
            down_local, hidden, (((1,), (1,)), ((), ())), preferred_element_type=jnp.float32
        ).astype(jnp.bfloat16),
        "tp",
        scatter_dimension=0,
        tiled=True,
    ).astype(jnp.float32)
    own_columns = summed.shape[0]
    outgoing_back = summed.astype(jnp.bfloat16).reshape(own_columns, fs_count, capacity)
    returned = lax.all_to_all(outgoing_back, "fs", split_axis=1, concat_axis=1, tiled=True).reshape(
        own_columns, experts * capacity
    )
    mixed = lax.dot_general(
        combine,
        returned.astype(jnp.float32),
        (((1,), (1,)), ((), ())),
        precision=lax.Precision.HIGHEST,
        preferred_element_type=jnp.float32,
    )
    return (mixed.astype(jnp.bfloat16), gate_new, up_new, down_new)


MESH = pl.DeviceIdType.MESH
STAGES = 2
QUARTERS = 4
ISSUE = (1, 2, 3)
EXPECTED = (7.0, 13.0, 16.0, 20.0, 22.0, 24.0, 28.0, 30.0, 32.0)
RETURN = 4


def flip(index, distance):
    bit = 1
    while bit <= distance:
        if distance & bit:
            index = index + bit - 2 * bit * ((index // bit) % 2)
        bit *= 2
    return index


def plan(works, pieces, chips):
    hop, pair = 4.7, 2.0
    starts, needs, now = [], [{}, {}], 0.0
    for w, (j, at, cost, sides) in enumerate(works):
        now = max(now, at)
        starts.append(now)
        now = now + cost
        for side in sides:
            needs[side][j] = (w, now)
    steps = [[[] for _ in range(chips)] for _ in works]
    before = [0.0] * pieces
    for p in range(chips):
        side, leave, floor = 2 * p // chips, 0.0, 0
        for j in range(pieces):
            w, done = needs[side][j]
            there = max(done + pair, before[j] + hop if p else 0.0)
            floor = max([floor, w] + [i for i, begin in enumerate(starts) if begin <= there])
            steps[floor][p].append(j)
            leave = max(leave + 1.0, there)
            before[j] = leave
    return steps


def rows_of(index, size):
    return pl.ds(pl.multiple_of(index * size, size), size)


def moe_kernel(
    fs,
    tp,
    tokens,
    gain,
    gate,
    up,
    down,
    route,
    route_weight,
    mixed,
    w_gate,
    w_up,
    w_down,
    gain_row,
    routes,
    weights_of,
    loaded,
    staged,
    tok,
    gated,
    up_acc,
    hidden,
    pair_own,
    pair_out,
    pair_in,
    chain_in,
    chain_out,
    back_in,
    share,
    mix_out,
    gain_col,
    load_sem,
    small_sem,
    tf_s,
    tf_r,
    az_s,
    az_r,
    as_s,
    as_r,
    w_s,
    g_r,
    u_r,
    dn_r,
    pr_s,
    pr_r,
    ch_s,
    ch_r,
    bk_s,
    bk_r,
    mx_s,
    mx_r,
):
    chips = tp // 2
    last = chips - 1
    f = lax.axis_index("fs")
    t = lax.axis_index("tp")
    z, core = t // 2, t % 2
    sibling = flip(t, 1)
    onward = t + 4 * core - 2
    place = core * z + (1 - core) * (last - z)
    strip, width = tokens.shape[1], tokens.shape[2]
    depth, units = gate.shape[1], gate.shape[2]
    block, rows_all = QUARTERS * strip, fs * QUARTERS * strip
    sub = width // STAGES
    piece_rows = fs * strip
    first = 1 - z // (chips // 2)
    sources, finals = (gate, up, down), (w_gate, w_up, w_down)

    barrier = pltpu.get_barrier_semaphore()
    for d in range(1, fs):
        pl.semaphore_signal(barrier, inc=1, device_id={"fs": flip(f, d)}, device_id_type=MESH)
    near = [1] + list(range(2, tp, 2))
    for d in near:
        pl.semaphore_signal(barrier, inc=1, device_id={"tp": flip(t, d)}, device_id_type=MESH)

    def tok_at(k, d):
        return tok.at[k, :, flip(f, d)]

    small = [
        pltpu.make_async_copy(source, target, small_sem.at[n])
        for n, (source, target) in enumerate(
            (
                (tokens, tok_at(t, 0)),
                (gain, gain_row),
                (route, routes),
                (route_weight, weights_of),
            )
        )
    ]
    for copy in small:
        copy.start()
    loads = {}

    def load(p, d):
        loads[p, d] = pltpu.make_async_copy(
            sources[p].at[flip(f, d)], loaded.at[p, d], load_sem.at[p, d]
        )
        loads[p, d].start()

    for d in ISSUE:
        load(0, d)
    for copy in small:
        copy.wait()
    pl.semaphore_wait(barrier, fs - 1 + len(near))

    def remote(src, dst, s_sem, r_sem, **device):
        return pltpu.make_async_remote_copy(
            src_ref=src,
            dst_ref=dst,
            send_sem=s_sem,
            recv_sem=r_sem,
            device_id=device,
            device_id_type=MESH,
        )

    def send(*args, **device):
        copy = remote(*args, **device)
        copy.start()
        return copy

    def send_if(condition, *args, **device):
        @pl.when(condition)
        def _():
            remote(*args, **device).start()

    def take(ref, sem):
        pltpu.make_async_copy(ref, ref, sem).wait()

    beside = ISSUE[:2]
    across = ISSUE[2]
    tok_fs = {
        d: send(tok_at(t, 0), tok_at(t, 0), tf_s, tf_r.at[d], fs=flip(f, d)) for d in beside
    }

    def tok_part(n, d):
        size = QUARTERS // 2
        return tok.at[t, pl.ds(n * size, size), flip(f, d)]

    def pass_on(n):
        piece = tok_part(n, beside[n])
        send(piece, piece, tf_s, tf_r.at[0 if n else across], fs=flip(f, beside[1 - n]))

    def spread(d):
        piece = tok_at(t, d)
        send_if(z < last, piece, piece, az_s.at[0], az_r.at[z, d], tp=t + 2)
        send_if(z > 0, piece, piece, az_s.at[1], az_r.at[z, d], tp=t - 2)
        send(piece, piece, as_s, as_r, tp=sibling)

    def relay(step, d):
        for way in range(2):
            towards = 1 - 2 * way
            here = (z >= step) if way == 0 else (z + step <= last)
            more = (z < last) if way == 0 else (z > 0)
            k = t - 2 * step * towards
            origin = z - step * towards
            piece = tok_at(k, d)

            @pl.when(here)
            def _():
                take(piece, az_r.at[origin, d])

            send_if(
                jnp.logical_and(here, more),
                piece,
                piece,
                az_s.at[way],
                az_r.at[origin, d],
                tp=t + 2 * towards,
            )
            send_if(here, piece, piece, as_s, as_r, tp=sibling)

    def cast(p, d):
        loads[p, d].wait()
        tile = 64

        @pl.loop(0, depth // tile)
        def _(i):
            rows = rows_of(i, tile)
            value = loaded[p, d, rows, :]
            if p < 2:
                value = value * gain_col[rows, 0:1]
            value = value.astype(jnp.bfloat16)
            if d:
                staged[p, d - 1, rows, :] = value
            else:
                finals[p][pl.ds(pl.multiple_of(f * depth + i * tile, tile), tile), :] = value

    arrive = {}

    def ship(p, d):
        cast(p, d)
        arrive[p, d] = send(
            staged.at[p, d - 1],
            finals[p].at[rows_of(f, depth)],
            w_s,
            u_r.at[d] if p else g_r,
            fs=flip(f, d),
        )

    spread(0)
    gain_col[...] = jnp.broadcast_to(gain_row[...], (128, depth)).T
    for d in ISSUE:
        load(1, d)
    for d in beside:
        ship(0, d)
    for d in ISSUE:
        load(2, d)
    for n, d in enumerate(beside):
        tok_fs[d].wait_recv()
        spread(d)
        pass_on(n)
    ship(0, across)
    for d in ISSUE:
        ship(1, d)
    for p in range(3):
        load(p, 0)
    for d in ISSUE:
        cast(2, d)
    def send_down(u, d, c, r_sem):
        send(
            staged.at[2, d - 1, pl.ds(pl.multiple_of(c * width + u * sub, sub), sub)],
            w_down.at[pl.ds(pl.multiple_of(f * depth + c * width + u * sub, sub), sub)],
            w_s,
            r_sem,
            fs=flip(f, d),
        )

    for u in range(STAGES - 1):
        for d in ISSUE:
            for c in range(2):
                send_down(u, d, c, dn_r.at[u, d])
    for side in range(2):
        for d in ISSUE:
            c = 1 - first if side else first
            send_down(STAGES - 1, d, c, dn_r.at[STAGES - 1 + side, d])
    for step in range(1, chips):
        for d in (0,) + beside:
            relay(step, d)
        if step == 1:
            for p in range(3):
                cast(p, 0)
            for e in range(fs):
                part = jnp.zeros((1, block), jnp.float32)
                for k in range(routes.shape[0]):
                    part = part + jnp.where(
                        routes[k : k + 1, :] == e, weights_of[k : k + 1, :], 0.0
                    )
                share[e] = jnp.broadcast_to(part, (sub, block)).T
        if step == chips - 2:
            for n in range(2):
                take(tok_part(n, across), tf_r.at[0 if n else across])
            spread(across)
    for step in range(1, chips):
        relay(step, across)
    take(tok.at[pl.ds(0, chips)], as_r)
    take(w_gate.at[pl.ds(0, (fs - 1) * depth)], g_r)

    def tok_rows(k, i):
        return tok[k, i].reshape(piece_rows, width)

    @pl.loop(0, QUARTERS)
    def _(i):
        rows = rows_of(i, piece_rows)
        parts = [tok_rows(k, i) for k in range(tp)]
        squares = jnp.zeros((piece_rows, 1), jnp.float32)
        for part in parts:
            value = part.astype(jnp.float32)
            squares = squares + jnp.sum(value * value, axis=1, keepdims=True)
        scale = lax.rsqrt(squares / (width * tp) + epsilon)
        acc = jnp.dot(
            jnp.concatenate(parts, axis=1), w_gate[...], preferred_element_type=jnp.float32
        )
        gated[rows, :] = jax.nn.silu(acc * scale) * scale

    def up_part(d, i):
        s = flip(f, d)
        value = jnp.concatenate([tok_rows(2 * s, i), tok_rows(2 * s + 1, i)], axis=1)
        return jnp.dot(value, w_up[rows_of(s, depth), :], preferred_element_type=jnp.float32)

    early = (0,) + ISSUE[:-1]
    for n, d in enumerate(early):
        if d:
            arrive[1, d].wait_recv()

        @pl.loop(0, QUARTERS)
        def _(i):
            rows = rows_of(i, piece_rows)
            part = up_part(d, i)
            up_acc[rows, :] = up_acc[rows, :] + part if n else part

    arrive[1, ISSUE[-1]].wait_recv()

    def finish_hidden(h):
        rows = pl.ds(h * piece_rows, piece_rows)
        value = up_acc[rows, :] + up_part(ISSUE[-1], h)
        hidden[rows, :] = (gated[rows, :] * value).astype(jnp.bfloat16)

    end = STAGES - 1
    pieces = [(u, 0, h) for h in range(QUARTERS) for u in range(STAGES)]
    pieces += [(u, d, h) for u in range(STAGES) for d in ISSUE for h in range(QUARTERS)]
    count = len(pieces)

    def product(j, side):
        u, d, h = pieces[j]
        s = flip(f, d)
        if d == 0 and u == 0:
            finish_hidden(h)
        if d and h == 0:
            size = 2 * sub if side is None else sub
            take(w_down.at[pl.ds(0, size)], dn_r.at[u + (side or 0), d])

        def weights(c):
            start = pl.multiple_of(s * depth + c * width + u * sub, sub)
            return w_down[pl.ds(start, sub), :]

        def times(weight):
            return lax.dot_general(
                hidden[pl.ds(h * piece_rows, piece_rows), :],
                weight,
                (((1,), (1,)), ((), ())),
                preferred_element_type=jnp.float32,
            )

        def give(value):
            pair_out[j] = value.astype(jnp.bfloat16)
            send(pair_out.at[j], pair_in.at[j], pr_s, pr_r.at[j], tp=sibling)

        if side is None:
            result = times(jnp.concatenate([weights(core), weights(1 - core)], axis=0))
            pair_own[j] = result[:, :sub]
            give(result[:, sub:])
            return
        c = 1 - first if side else first
        result = times(weights(c))

        @pl.when(core == c)
        def _():
            pair_own[j] = result

        @pl.when(core != c)
        def _():
            give(result)

    def advance(p, j):
        u, d, h = pieces[j]
        s = flip(f, d)
        take(pair_in.at[j], pr_r.at[j])
        if p:
            take(chain_in.at[j], ch_r.at[j])

        value = pair_own[j] + pair_in[j].astype(jnp.float32)
        if p:
            value = value + chain_in[j].astype(jnp.float32)
        chain_out[j] = value.astype(jnp.bfloat16)

        if p < last:
            send(chain_out.at[j], chain_in.at[j], ch_s, ch_r.at[j], tp=onward)
            return
        for b in range(fs):
            rows = pl.ds(b * strip, strip)

            @pl.when(f != b)
            def _():
                send(chain_out.at[j, rows], back_in.at[u, h, s, f], bk_s, bk_r.at[u, h], fs=b)

            @pl.when(f == b)
            def _():
                back_in[u, h, s, f] = chain_out[j, rows, :]

    def combine(u, h):
        take(back_in.at[u, h, :, pl.ds(0, fs - 1)], bk_r.at[u, h])
        for s in range(fs):
            value = jnp.zeros((strip, sub), jnp.float32)
            for e in range(fs):
                value = value + share[e, pl.ds(h * strip, strip), :] * back_in[u, h, s, e].astype(
                    jnp.float32
                )
            value = value.astype(jnp.bfloat16)

            @pl.when(s == z)
            def _():
                mixed[u, h] = value

            @pl.when(s != z)
            def _():
                mix_out[u, h, s] = value
                send(mix_out.at[u, h, s], mixed.at[u, h], mx_s, mx_r.at[u, h], tp=2 * s + core)

    works = [(j, 0.0, 0.5 if pieces[j][0] else 1.0, (0, 1)) for j in range(STAGES * QUARTERS)]
    times_of = iter(EXPECTED)
    index = {piece: j for j, piece in enumerate(pieces)}
    for u in range(STAGES):
        for side in (0, 1) if u == end else (None,):
            for d in ISSUE:
                at = next(times_of)
                sides = (0, 1) if side is None else (side,)
                works += [(index[u, d, h], at, 0.5, sides) for h in range(QUARTERS)]
    steps = plan(works, count, chips)
    split = {j for j in range(count) if pieces[j][0] == end and pieces[j][1]}
    waiting = [(u, h) for u in range(STAGES) for h in range(QUARTERS)]
    for w, (j, _, _, sides) in enumerate(works):
        product(j, sides[0] if j in split else None)
        for p in range(chips):
            if not steps[w][p]:
                continue

            @pl.when(place == p)
            def _():
                for i in steps[w][p]:
                    advance(p, i)
                    if p == last and waiting[0][0] < end and i >= count - len(split) + RETURN:
                        combine(*waiting.pop(0))

    @pl.when(place == last)
    def _():
        for u, h in waiting:
            combine(u, h)

    @pl.when(place < last)
    def _():
        for u in range(STAGES):
            for h in range(QUARTERS):
                take(mixed.at[u, h], mx_r.at[u, h])

    take(tok.at[0, :, pl.ds(0, fs - 1)], tf_s)
    for n in range(chips):

        @pl.when(z == n)
        def _():
            if n < last:
                take(tok.at[pl.ds(0, 1 + n)], az_s.at[0])
            if n:
                take(tok.at[pl.ds(0, chips - n)], az_s.at[1])

    take(tok.at[pl.ds(0, chips)], as_s)
    take(staged, w_s)
    take(pair_out, pr_s)

    @pl.when(place < last)
    def _():
        take(chain_out, ch_s)

    @pl.when(place == last)
    def _():
        take(back_in.at[:, :, :, pl.ds(0, fs - 1)], bk_s)
        take(mix_out.at[:, :, pl.ds(0, chips - 1)], mx_s)


def write_kernel(mixed, gate, up, down, mixed_out, gate_out, up_out, down_out, sem):
    sub = mixed.shape[3]
    copies = [
        pltpu.make_async_copy(mixed.at[u], mixed_out.at[:, :, pl.ds(u * sub, sub)], sem.at[u])
        for u in range(STAGES)
    ]
    pairs = ((gate, gate_out), (up, up_out), (down, down_out))
    copies += [
        pltpu.make_async_copy(source, target.at[0], sem.at[STAGES + n])
        for n, (source, target) in enumerate(pairs)
    ]
    for copy in copies:
        copy.start()
    for copy in copies:
        copy.wait()


def write_out(mixed, *weights):
    whole = pl.BlockSpec(memory_space=pltpu.VMEM)
    far = pl.BlockSpec(memory_space=pl.ANY)
    stages, quarters, strip, sub = mixed.shape
    shapes = [jax.ShapeDtypeStruct((quarters, strip, stages * sub), mixed.dtype)]
    shapes += [jax.ShapeDtypeStruct((1,) + w.shape, w.dtype) for w in weights]
    mixed, *weights = pl.pallas_call(
        write_kernel,
        out_shape=tuple(shapes),
        in_specs=[whole] * len(shapes),
        out_specs=tuple([far] * len(shapes)),
        scratch_shapes=[pltpu.SemaphoreType.DMA((stages + len(weights),))],
        compiler_params=pltpu.CompilerParams(vmem_limit_bytes=1024 * 1024),
    )(mixed, *weights)
    return (mixed.reshape(quarters * strip, stages * sub), *weights)


def dense_body(tokens, norm_gain, gate_weight, up_weight, down_weight, route, route_weight):
    fs, tp = lax.axis_size("fs"), lax.axis_size("tp")
    block, width = tokens.shape
    experts, depth, units = gate_weight.shape
    rows, full, sub, chips = fs * block, tp * width, width // STAGES, tp // 2
    count, strip = STAGES * fs * QUARTERS, block // QUARTERS
    piece = fs * strip
    whole = pl.BlockSpec(memory_space=pltpu.VMEM)
    far = pl.BlockSpec(memory_space=pl.ANY)
    narrow, wide, dma = jnp.bfloat16, jnp.float32, pltpu.SemaphoreType.DMA
    weight = pltpu.VMEM((full, units), narrow)
    mixed, gate_new, up_new, down_new = pl.pallas_call(
        functools.partial(moe_kernel, fs, tp),
        out_shape=(pltpu.VMEM((STAGES, QUARTERS, strip, sub), narrow), weight, weight, weight),
        in_specs=[far] * 7,
        out_specs=(whole, whole, whole, whole),
        scratch_shapes=[
            pltpu.VMEM((1, depth), wide),
            pltpu.VMEM((route.shape[1], block), jnp.int32),
            pltpu.VMEM((route.shape[1], block), wide),
            pltpu.VMEM((3, experts, depth, units), wide),
            pltpu.VMEM((3, fs - 1, depth, units), narrow),
            pltpu.VMEM((tp, QUARTERS, fs, strip, width), narrow),
            pltpu.VMEM((rows, units), wide),
            pltpu.VMEM((rows, units), wide),
            pltpu.VMEM((rows, units), narrow),
            pltpu.VMEM((count, piece, sub), wide),
            pltpu.VMEM((count, piece, sub), narrow),
            pltpu.VMEM((count, piece, sub), narrow),
            pltpu.VMEM((count, piece, sub), narrow),
            pltpu.VMEM((count, piece, sub), narrow),
            pltpu.VMEM((STAGES, QUARTERS, fs, fs, strip, sub), narrow),
            pltpu.VMEM((fs, block, sub), wide),
            pltpu.VMEM((STAGES, QUARTERS, fs, strip, sub), narrow),
            pltpu.VMEM((depth, 128), wide),
            dma((3, experts)),
            dma((4,)),
            dma,
            dma((fs,)),
            dma((2,)),
            dma((chips, fs)),
            dma,
            dma,
            dma,
            dma,
            dma((fs,)),
            dma((STAGES + 1, fs)),
            dma,
            dma((count,)),
            dma,
            dma((count,)),
            dma,
            dma((STAGES, QUARTERS)),
            dma,
            dma((STAGES, QUARTERS)),
        ],
        compiler_params=pltpu.CompilerParams(
            collective_id=0, has_side_effects=True, vmem_limit_bytes=56 * 1024 * 1024
        ),
    )(
        tokens.reshape(QUARTERS, strip, width),
        norm_gain[None, :],
        gate_weight,
        up_weight,
        down_weight,
        route.T,
        route_weight.T,
    )
    return write_out(mixed, gate_new, up_new, down_new)


def body(tokens, norm_gain, gate_weight, up_weight, down_weight, route, route_weight):
    fs, tp = lax.axis_size("fs"), lax.axis_size("tp")
    fits = (
        fs == 4
        and tp == 2 * fs
        and gate_weight.shape[0] == fs
        and tokens.shape[1] % (128 * STAGES) == 0
        and tokens.shape[0] % (64 * QUARTERS) == 0
        and gate_weight.shape[1] == 2 * tokens.shape[1]
        and tokens.shape[0] * fs * tokens.shape[1] * tp <= 1024 * 2048
    )
    chosen = dense_body if fits else slotted_body
    return chosen(tokens, norm_gain, gate_weight, up_weight, down_weight, route, route_weight)


def solution(mesh):
    in_specs = (
        P("fs", "tp"),
        P("fs"),
        P(None, "fs", "tp"),
        P(None, "fs", "tp"),
        P(None, "fs", "tp"),
        P("fs", None),
        P("fs", None),
    )
    out_specs = (P("fs", "tp"), P("fs", None, "tp"), P("fs", None, "tp"), P("fs", None, "tp"))
    return jax.shard_map(body, mesh=mesh, in_specs=in_specs, out_specs=out_specs, check_vma=False)
```

```python
import functools

import jax
import jax.numpy as jnp
from jax import lax
from jax.experimental import pallas as pl
from jax.experimental.pallas import tpu as pltpu
from jax.sharding import PartitionSpec as P

epsilon = 1e-05


def slot_table(route, block_rows, expert_count):
    pair_ids = route.reshape(-1, block_rows * route.shape[1])
    onehot = (
        pair_ids[:, :, None] == jnp.arange(expert_count, dtype=jnp.int32)[None, None, :]
    ).astype(jnp.int32)
    before = jnp.cumsum(onehot, axis=1) - onehot
    return jnp.sum(before * onehot, axis=2).reshape(route.shape)


def slotted_body(tokens, norm_gain, gate_weight, up_weight, down_weight, route, route_weight):
    experts = gate_weight.shape[0]
    tok_rows = tokens.shape[0]
    columns = tokens.shape[1]
    fs_count = lax.axis_size("fs")
    capacity = 4 * tok_rows // fs_count
    gain_col = norm_gain[None, :, None]
    gate_cast = (gate_weight * gain_col).astype(jnp.bfloat16)
    up_cast = (up_weight * gain_col).astype(jnp.bfloat16)
    down_cast = down_weight.astype(jnp.bfloat16)
    gate_new, up_new, down_new = (
        lax.all_to_all(gate_cast, "fs", split_axis=0, concat_axis=1, tiled=True),
        lax.all_to_all(up_cast, "fs", split_axis=0, concat_axis=1, tiled=True),
        lax.all_to_all(down_cast, "fs", split_axis=0, concat_axis=1, tiled=True),
    )
    slot_of = slot_table(route, tok_rows, experts)
    target = route * capacity + slot_of
    slot_lanes = jnp.arange(experts * capacity, dtype=jnp.int32)
    slot_hits = target[:, :, None] == slot_lanes[None, None, :]
    token_iota = jnp.arange(tok_rows, dtype=jnp.int32)[:, None, None]
    lane_token = jnp.sum(jnp.where(slot_hits, token_iota + 1, 0), axis=(0, 1)) - 1
    lane_token = jnp.where(lane_token < 0, tok_rows, lane_token)
    combine = jnp.sum(jnp.where(slot_hits, route_weight[:, :, None], 0.0), axis=1)
    tok_float = tokens.astype(jnp.float32)
    square_sum = lax.psum(jnp.sum(tok_float * tok_float, axis=1), "tp")
    full_width = columns * lax.axis_size("tp")
    normed = (tok_float * lax.rsqrt(square_sum / full_width + epsilon)[:, None]).astype(
        jnp.bfloat16
    )
    padded = jnp.concatenate([normed, jnp.zeros((1, columns), jnp.bfloat16)], axis=0)
    outgoing = padded[lane_token].reshape(experts, capacity, columns)
    arrived = lax.all_to_all(outgoing, "fs", split_axis=0, concat_axis=0, tiled=True).reshape(
        -1, columns
    )
    gate_local = gate_new[0]
    up_local = up_new[0]
    piece_rows = lax.all_gather(arrived, "tp", axis=1, tiled=True)
    gate_acc = jnp.dot(piece_rows, gate_local, preferred_element_type=jnp.float32)
    up_acc = jnp.dot(piece_rows, up_local, preferred_element_type=jnp.float32)
    hidden = (jax.nn.silu(gate_acc) * up_acc).astype(jnp.bfloat16)
    down_local = down_new[0]
    summed = lax.psum_scatter(
        lax.dot_general(
            down_local, hidden, (((1,), (1,)), ((), ())), preferred_element_type=jnp.float32
        ).astype(jnp.bfloat16),
        "tp",
        scatter_dimension=0,
        tiled=True,
    ).astype(jnp.float32)
    own_columns = summed.shape[0]
    outgoing_back = summed.astype(jnp.bfloat16).reshape(own_columns, fs_count, capacity)
    returned = lax.all_to_all(outgoing_back, "fs", split_axis=1, concat_axis=1, tiled=True).reshape(
        own_columns, experts * capacity
    )
    mixed = lax.dot_general(
        combine,
        returned.astype(jnp.float32),
        (((1,), (1,)), ((), ())),
        precision=lax.Precision.HIGHEST,
        preferred_element_type=jnp.float32,
    )
    return (mixed.astype(jnp.bfloat16), gate_new, up_new, down_new)


MESH = pl.DeviceIdType.MESH
STAGES = 2
QUARTERS = 4
ISSUE = (1, 2, 3)
EXPECTED = (7.0, 13.5, 16.0, 19.0, 22.0, 24.0, 27.0, 30.5, 32.0)


def flip(index, distance):
    bit = 1
    while bit <= distance:
        if distance & bit:
            index = index + bit - 2 * bit * ((index // bit) % 2)
        bit *= 2
    return index


def plan(works, chain, chips):
    hop, pair = 4.7, 2.0
    starts, needs, now = [], [{}, {}], 0.0
    for w, (j, at, cost, sides) in enumerate(works):
        now = max(now, at)
        starts.append(now)
        now = now + cost
        for side in sides:
            needs[side][j] = (w, now)
    steps = [[[] for _ in range(chips)] for _ in works]
    before = {}
    for p in range(chips):
        side, leave, floor = 2 * p // chips, 0.0, 0
        for j in chain:
            w, done = needs[side][j]
            there = max(done + pair, before[j] + hop if p else 0.0)
            floor = max([floor, w] + [i for i, begin in enumerate(starts) if begin <= there])
            steps[floor][p].append(j)
            leave = max(leave + 1.0, there)
            before[j] = leave
    return steps


def rows_of(index, size):
    return pl.ds(pl.multiple_of(index * size, size), size)


def moe_kernel(
    fs,
    tp,
    tokens,
    gain,
    gate,
    up,
    down,
    route,
    route_weight,
    mixed,
    w_gate,
    w_up,
    w_down,
    gain_row,
    routes,
    weights_of,
    loaded,
    staged,
    tok,
    gated,
    up_acc,
    hidden,
    pair_own,
    pair_out,
    pair_in,
    chain_in,
    chain_out,
    back_in,
    share,
    mix_out,
    side_in,
    part_out,
    part_in,
    gain_col,
    load_sem,
    small_sem,
    tf_s,
    tf_r,
    az_s,
    az_r,
    as_s,
    as_r,
    w_s,
    g_r,
    u_r,
    dn_r,
    pr_s,
    pr_r,
    ch_s,
    ch_r,
    bk_s,
    bk_r,
    mx_s,
    mx_r,
    sd_s,
    sd_r,
    pt_s,
    pt_r,
):
    chips = tp // 2
    last = chips - 1
    f = lax.axis_index("fs")
    t = lax.axis_index("tp")
    z, core = t // 2, t % 2
    sibling = flip(t, 1)
    onward = t + 4 * core - 2
    place = core * z + (1 - core) * (last - z)
    strip, width = tokens.shape[1], tokens.shape[2]
    depth, units = gate.shape[1], gate.shape[2]
    block, rows_all = QUARTERS * strip, fs * QUARTERS * strip
    sub = width // STAGES
    piece_rows = fs * strip
    first = 1 - z // (chips // 2)
    sources, finals = (gate, up, down), (w_gate, w_up, w_down)

    barrier = pltpu.get_barrier_semaphore()
    for d in range(1, fs):
        pl.semaphore_signal(barrier, inc=1, device_id={"fs": flip(f, d)}, device_id_type=MESH)
        beyond = {"fs": flip(f, d), "tp": sibling}
        pl.semaphore_signal(barrier, inc=1, device_id=beyond, device_id_type=MESH)
    near = [1] + list(range(2, tp, 2))
    for d in near:
        pl.semaphore_signal(barrier, inc=1, device_id={"tp": flip(t, d)}, device_id_type=MESH)

    def tok_at(k, d):
        return tok.at[k, :, flip(f, d)]

    small = [
        pltpu.make_async_copy(source, target, small_sem.at[n])
        for n, (source, target) in enumerate(
            (
                (tokens, tok_at(t, 0)),
                (gain, gain_row),
                (route, routes),
                (route_weight, weights_of),
            )
        )
    ]
    for copy in small:
        copy.start()
    loads = {}

    def load(p, d):
        loads[p, d] = pltpu.make_async_copy(
            sources[p].at[flip(f, d)], loaded.at[p, d], load_sem.at[p, d]
        )
        loads[p, d].start()

    for d in ISSUE:
        load(0, d)
    for copy in small:
        copy.wait()
    pl.semaphore_wait(barrier, 2 * (fs - 1) + len(near))

    def remote(src, dst, s_sem, r_sem, **device):
        return pltpu.make_async_remote_copy(
            src_ref=src,
            dst_ref=dst,
            send_sem=s_sem,
            recv_sem=r_sem,
            device_id=device,
            device_id_type=MESH,
        )

    def send(*args, **device):
        copy = remote(*args, **device)
        copy.start()
        return copy

    def send_if(condition, *args, **device):
        @pl.when(condition)
        def _():
            remote(*args, **device).start()

    def take(ref, sem):
        pltpu.make_async_copy(ref, ref, sem).wait()

    beside = ISSUE[:2]
    across = ISSUE[2]
    tok_fs = {
        d: send(tok_at(t, 0), tok_at(t, 0), tf_s, tf_r.at[d], fs=flip(f, d)) for d in beside
    }

    def tok_part(n, d):
        size = QUARTERS // 2
        return tok.at[t, pl.ds(n * size, size), flip(f, d)]

    def pass_on(n):
        piece = tok_part(n, beside[n])
        send(piece, piece, tf_s, tf_r.at[0 if n else across], fs=flip(f, beside[1 - n]))

    def spread(d):
        piece = tok_at(t, d)
        send_if(z < last, piece, piece, az_s.at[0], az_r.at[z, d], tp=t + 2)
        send_if(z > 0, piece, piece, az_s.at[1], az_r.at[z, d], tp=t - 2)
        send(piece, piece, as_s, as_r, tp=sibling)

    def relay(step, d):
        for way in range(2):
            towards = 1 - 2 * way
            here = (z >= step) if way == 0 else (z + step <= last)
            more = (z < last) if way == 0 else (z > 0)
            k = t - 2 * step * towards
            origin = z - step * towards
            piece = tok_at(k, d)

            @pl.when(here)
            def _():
                take(piece, az_r.at[origin, d])

            send_if(
                jnp.logical_and(here, more),
                piece,
                piece,
                az_s.at[way],
                az_r.at[origin, d],
                tp=t + 2 * towards,
            )
            send_if(here, piece, piece, as_s, as_r, tp=sibling)

    def cast(p, d):
        loads[p, d].wait()
        tile = 64

        @pl.loop(0, depth // tile)
        def _(i):
            rows = rows_of(i, tile)
            value = loaded[p, d, rows, :]
            if p < 2:
                value = value * gain_col[rows, 0:1]
            value = value.astype(jnp.bfloat16)
            if d:
                staged[p, d - 1, rows, :] = value
            else:
                finals[p][pl.ds(pl.multiple_of(f * depth + i * tile, tile), tile), :] = value

    arrive = {}

    def ship(p, d):
        cast(p, d)
        arrive[p, d] = send(
            staged.at[p, d - 1],
            finals[p].at[rows_of(f, depth)],
            w_s,
            u_r.at[d] if p else g_r,
            fs=flip(f, d),
        )

    spread(0)
    gain_col[...] = jnp.broadcast_to(gain_row[...], (128, depth)).T
    for d in ISSUE:
        load(1, d)
    for d in beside:
        ship(0, d)
    for d in ISSUE:
        load(2, d)
    for n, d in enumerate(beside):
        tok_fs[d].wait_recv()
        spread(d)
        pass_on(n)
    ship(0, across)
    for d in ISSUE:
        ship(1, d)
    for p in range(3):
        load(p, 0)
    for d in ISSUE:
        cast(2, d)
    def send_down(u, d, c, r_sem):
        send(
            staged.at[2, d - 1, pl.ds(pl.multiple_of(c * width + u * sub, sub), sub)],
            w_down.at[pl.ds(pl.multiple_of(f * depth + c * width + u * sub, sub), sub)],
            w_s,
            r_sem,
            fs=flip(f, d),
        )

    for u in range(STAGES - 1):
        for d in ISSUE:
            for c in range(2):
                send_down(u, d, c, dn_r.at[u, d])
    for side in range(2):
        for d in ISSUE:
            c = 1 - first if side else first
            send_down(STAGES - 1, d, c, dn_r.at[STAGES - 1 + side, d])
    for step in range(1, chips):
        for d in (0,) + beside:
            relay(step, d)
        if step == 1:
            for p in range(3):
                cast(p, 0)
            for e in range(fs):
                part = jnp.zeros((1, block), jnp.float32)
                for k in range(routes.shape[0]):
                    part = part + jnp.where(
                        routes[k : k + 1, :] == e, weights_of[k : k + 1, :], 0.0
                    )
                share[e] = jnp.broadcast_to(part, (sub, block)).T
        if step == chips - 2:
            for n in range(2):
                take(tok_part(n, across), tf_r.at[0 if n else across])
            spread(across)
    for step in range(1, chips):
        relay(step, across)
    take(tok.at[pl.ds(0, chips)], as_r)
    take(w_gate.at[pl.ds(0, (fs - 1) * depth)], g_r)

    def tok_rows(k, i):
        return tok[k, i].reshape(piece_rows, width)

    @pl.loop(0, QUARTERS)
    def _(i):
        rows = rows_of(i, piece_rows)
        parts = [tok_rows(k, i) for k in range(tp)]
        squares = jnp.zeros((piece_rows, 1), jnp.float32)
        for part in parts:
            value = part.astype(jnp.float32)
            squares = squares + jnp.sum(value * value, axis=1, keepdims=True)
        scale = lax.rsqrt(squares / (width * tp) + epsilon)
        acc = jnp.dot(
            jnp.concatenate(parts, axis=1), w_gate[...], preferred_element_type=jnp.float32
        )
        gated[rows, :] = jax.nn.silu(acc * scale) * scale

    def up_part(d, i):
        s = flip(f, d)
        value = jnp.concatenate([tok_rows(2 * s, i), tok_rows(2 * s + 1, i)], axis=1)
        return jnp.dot(value, w_up[rows_of(s, depth), :], preferred_element_type=jnp.float32)

    early = (0,) + ISSUE[:-1]
    for n, d in enumerate(early):
        if d:
            arrive[1, d].wait_recv()

        @pl.loop(0, QUARTERS)
        def _(i):
            rows = rows_of(i, piece_rows)
            part = up_part(d, i)
            up_acc[rows, :] = up_acc[rows, :] + part if n else part

    arrive[1, ISSUE[-1]].wait_recv()

    def finish_hidden(h):
        rows = pl.ds(h * piece_rows, piece_rows)
        value = up_acc[rows, :] + up_part(ISSUE[-1], h)
        hidden[rows, :] = (gated[rows, :] * value).astype(jnp.bfloat16)

    end = STAGES - 1
    pieces = [(u, 0, h) for h in range(QUARTERS) for u in range(STAGES)]
    pieces += [(u, d, h) for u in range(STAGES) for d in ISSUE for h in range(QUARTERS)]
    count = len(pieces)
    late = QUARTERS - 1
    chain = [j for j, (u, _, h) in enumerate(pieces) if u < end or h < late]

    def product(j, side):
        u, d, h = pieces[j]
        s = flip(f, d)
        if d == 0 and u == 0:
            finish_hidden(h)
        if d and h == 0:
            size = 2 * sub if side is None else sub
            take(w_down.at[pl.ds(0, size)], dn_r.at[u + (side or 0), d])

        def weights(c):
            start = pl.multiple_of(s * depth + c * width + u * sub, sub)
            return w_down[pl.ds(start, sub), :]

        def times(weight):
            return lax.dot_general(
                hidden[pl.ds(h * piece_rows, piece_rows), :],
                weight,
                (((1,), (1,)), ((), ())),
                preferred_element_type=jnp.float32,
            )

        def give(value):
            pair_out[j] = value.astype(jnp.bfloat16)
            send(pair_out.at[j], pair_in.at[j], pr_s, pr_r.at[j], tp=sibling)

        if side is None:
            result = times(jnp.concatenate([weights(core), weights(1 - core)], axis=0))
            pair_own[j] = result[:, :sub]
            give(result[:, sub:])
            return
        c = 1 - first if side else first
        result = times(weights(c))

        @pl.when(core == c)
        def _():
            pair_own[j] = result

        @pl.when(core != c)
        def _():
            give(result)

    def advance(p, j):
        u, d, h = pieces[j]
        s = flip(f, d)
        take(pair_in.at[j], pr_r.at[j])
        if p:
            take(chain_in.at[j], ch_r.at[j])

        value = pair_own[j] + pair_in[j].astype(jnp.float32)
        if p:
            value = value + chain_in[j].astype(jnp.float32)
        chain_out[j] = value.astype(jnp.bfloat16)

        if p < last:
            send(chain_out.at[j], chain_in.at[j], ch_s, ch_r.at[j], tp=onward)
            return
        for b in range(fs):
            rows = pl.ds(b * strip, strip)
            send(
                chain_out.at[j, rows],
                back_in.at[u, h, s, f],
                bk_s,
                bk_r.at[u, h],
                fs=b,
                tp=sibling,
            )

    def mix(shares, h):
        value = jnp.zeros((strip, sub), jnp.float32)
        for e in range(fs):
            rows = pl.ds(h * strip, strip)
            value = value + share[e, rows, :] * shares[e].astype(jnp.float32)
        return value.astype(jnp.bfloat16)

    def combine(u, h):
        take(back_in.at[u, h], bk_r.at[u, h])
        for s in range(fs):
            mix_out[u, h, s] = mix([back_in[u, h, s, e] for e in range(fs)], h)
            send(
                mix_out.at[u, h, s], mixed.at[u, h], mx_s, mx_r.at[u, h], tp=2 * s + 1 - core
            )

    def offer():
        for d in (0,) + ISSUE:
            j = index[end, d, late]
            s = flip(f, d)
            take(pair_in.at[j], pr_r.at[j])
            value = pair_own[j] + pair_in[j].astype(jnp.float32)
            chain_out[j] = value.astype(jnp.bfloat16)
            for b in range(fs):
                rows = pl.ds(b * strip, strip)

                @pl.when(f != b)
                def _():
                    send(chain_out.at[j, rows], side_in.at[s, f], sd_s, sd_r, fs=b)

                @pl.when(f == b)
                def _():
                    side_in[s, f] = chain_out[j, rows, :]

    def settle():
        take(side_in.at[:, pl.ds(0, fs - 1)], sd_r)
        for s in range(fs):
            value = mix([side_in[s, e] for e in range(fs)], late)

            @pl.when(s == z)
            def _():
                part_in[s] = value

            @pl.when(s != z)
            def _():
                part_out[s] = value
                send(part_out.at[s], part_in.at[z], pt_s, pt_r, tp=2 * s + core)

    def close():
        take(part_in.at[pl.ds(0, chips - 1)], pt_r)
        value = jnp.zeros((strip, sub), jnp.float32)
        for k in range(chips):
            value = value + part_in[k].astype(jnp.float32)
        mixed[end, late] = value.astype(jnp.bfloat16)

    works = [(j, 0.0, 0.5 if pieces[j][0] else 1.0, (0, 1)) for j in range(STAGES * QUARTERS)]
    times_of = iter(EXPECTED)
    index = {piece: j for j, piece in enumerate(pieces)}
    for u in range(STAGES):
        for side in (0, 1) if u == end else (None,):
            for d in ISSUE:
                at = next(times_of)
                sides = (0, 1) if side is None else (side,)
                works += [(index[u, d, h], at, 0.5, sides) for h in range(QUARTERS)]
    steps = plan(works, chain, chips)
    split = {j for j in range(count) if pieces[j][0] == end and pieces[j][1]}
    for w, (j, _, _, sides) in enumerate(works):
        product(j, sides[0] if j in split else None)
        for p in range(chips):
            todo = steps[w][p]
            if not todo and w < len(works) - 1:
                continue

            @pl.when(place == p)
            def _():
                for i in todo[:2]:
                    advance(p, i)
                if w == len(works) - 1:
                    offer()
                for i in todo[2:]:
                    advance(p, i)

    placed = [(u, h) for u in range(STAGES) for h in range(QUARTERS) if u < end or h < late]

    @pl.when(place == 0)
    def _():
        for u, h in placed:
            if u < end:
                combine(u, h)

    settle()

    @pl.when(place == 0)
    def _():
        for u, h in placed:
            if u == end:
                combine(u, h)

    close()
    for u, h in placed:
        take(mixed.at[u, h], mx_r.at[u, h])

    take(tok.at[0, :, pl.ds(0, fs - 1)], tf_s)
    for n in range(chips):

        @pl.when(z == n)
        def _():
            if n < last:
                take(tok.at[pl.ds(0, 1 + n)], az_s.at[0])
            if n:
                take(tok.at[pl.ds(0, chips - n)], az_s.at[1])

    take(tok.at[pl.ds(0, chips)], as_s)
    take(staged, w_s)
    take(pair_out, pr_s)

    take(side_in.at[:, pl.ds(0, fs - 1)], sd_s)
    take(part_out.at[pl.ds(0, chips - 1)], pt_s)
    passed = chain_out.at[pl.ds(0, len(chain))]

    @pl.when(place < last)
    def _():
        take(passed, ch_s)

    @pl.when(place == last)
    def _():
        take(passed, bk_s)

    @pl.when(place == 0)
    def _():
        take(chain_out.at[pl.ds(0, len(placed))], mx_s)


def write_kernel(mixed, gate, up, down, mixed_out, gate_out, up_out, down_out, sem):
    sub = mixed.shape[3]
    copies = [
        pltpu.make_async_copy(mixed.at[u], mixed_out.at[:, :, pl.ds(u * sub, sub)], sem.at[u])
        for u in range(STAGES)
    ]
    pairs = ((gate, gate_out), (up, up_out), (down, down_out))
    copies += [
        pltpu.make_async_copy(source, target.at[0], sem.at[STAGES + n])
        for n, (source, target) in enumerate(pairs)
    ]
    for copy in copies:
        copy.start()
    for copy in copies:
        copy.wait()


def write_out(mixed, *weights):
    whole = pl.BlockSpec(memory_space=pltpu.VMEM)
    far = pl.BlockSpec(memory_space=pl.ANY)
    stages, quarters, strip, sub = mixed.shape
    shapes = [jax.ShapeDtypeStruct((quarters, strip, stages * sub), mixed.dtype)]
    shapes += [jax.ShapeDtypeStruct((1,) + w.shape, w.dtype) for w in weights]
    mixed, *weights = pl.pallas_call(
        write_kernel,
        out_shape=tuple(shapes),
        in_specs=[whole] * len(shapes),
        out_specs=tuple([far] * len(shapes)),
        scratch_shapes=[pltpu.SemaphoreType.DMA((stages + len(weights),))],
        compiler_params=pltpu.CompilerParams(vmem_limit_bytes=1024 * 1024),
    )(mixed, *weights)
    return (mixed.reshape(quarters * strip, stages * sub), *weights)


def dense_body(tokens, norm_gain, gate_weight, up_weight, down_weight, route, route_weight):
    fs, tp = lax.axis_size("fs"), lax.axis_size("tp")
    block, width = tokens.shape
    experts, depth, units = gate_weight.shape
    rows, full, sub, chips = fs * block, tp * width, width // STAGES, tp // 2
    count, strip = STAGES * fs * QUARTERS, block // QUARTERS
    piece = fs * strip
    whole = pl.BlockSpec(memory_space=pltpu.VMEM)
    far = pl.BlockSpec(memory_space=pl.ANY)
    narrow, wide, dma = jnp.bfloat16, jnp.float32, pltpu.SemaphoreType.DMA
    weight = pltpu.VMEM((full, units), narrow)
    mixed, gate_new, up_new, down_new = pl.pallas_call(
        functools.partial(moe_kernel, fs, tp),
        out_shape=(pltpu.VMEM((STAGES, QUARTERS, strip, sub), narrow), weight, weight, weight),
        in_specs=[far] * 7,
        out_specs=(whole, whole, whole, whole),
        scratch_shapes=[
            pltpu.VMEM((1, depth), wide),
            pltpu.VMEM((route.shape[1], block), jnp.int32),
            pltpu.VMEM((route.shape[1], block), wide),
            pltpu.VMEM((3, experts, depth, units), wide),
            pltpu.VMEM((3, fs - 1, depth, units), narrow),
            pltpu.VMEM((tp, QUARTERS, fs, strip, width), narrow),
            pltpu.VMEM((rows, units), wide),
            pltpu.VMEM((rows, units), wide),
            pltpu.VMEM((rows, units), narrow),
            pltpu.VMEM((count, piece, sub), wide),
            pltpu.VMEM((count, piece, sub), narrow),
            pltpu.VMEM((count, piece, sub), narrow),
            pltpu.VMEM((count, piece, sub), narrow),
            pltpu.VMEM((count, piece, sub), narrow),
            pltpu.VMEM((STAGES, QUARTERS, fs, fs, strip, sub), narrow),
            pltpu.VMEM((fs, block, sub), wide),
            pltpu.VMEM((STAGES, QUARTERS, fs, strip, sub), narrow),
            pltpu.VMEM((fs, fs, strip, sub), narrow),
            pltpu.VMEM((fs, strip, sub), narrow),
            pltpu.VMEM((chips, strip, sub), narrow),
            pltpu.VMEM((depth, 128), wide),
            dma((3, experts)),
            dma((4,)),
            dma,
            dma((fs,)),
            dma((2,)),
            dma((chips, fs)),
            dma,
            dma,
            dma,
            dma,
            dma((fs,)),
            dma((STAGES + 1, fs)),
            dma,
            dma((count,)),
            dma,
            dma((count,)),
            dma,
            dma((STAGES, QUARTERS)),
            dma,
            dma((STAGES, QUARTERS)),
            dma,
            dma,
            dma,
            dma,
        ],
        compiler_params=pltpu.CompilerParams(
            collective_id=0, has_side_effects=True, vmem_limit_bytes=56 * 1024 * 1024
        ),
    )(
        tokens.reshape(QUARTERS, strip, width),
        norm_gain[None, :],
        gate_weight,
        up_weight,
        down_weight,
        route.T,
        route_weight.T,
    )
    return write_out(mixed, gate_new, up_new, down_new)


def body(tokens, norm_gain, gate_weight, up_weight, down_weight, route, route_weight):
    fs, tp = lax.axis_size("fs"), lax.axis_size("tp")
    fits = (
        fs == 4
        and tp == 2 * fs
        and gate_weight.shape[0] == fs
        and tokens.shape[1] % (128 * STAGES) == 0
        and tokens.shape[0] % (64 * QUARTERS) == 0
        and gate_weight.shape[1] == 2 * tokens.shape[1]
        and tokens.shape[0] * fs * tokens.shape[1] * tp <= 1024 * 2048
    )
    chosen = dense_body if fits else slotted_body
    return chosen(tokens, norm_gain, gate_weight, up_weight, down_weight, route, route_weight)


def solution(mesh):
    in_specs = (
        P("fs", "tp"),
        P("fs"),
        P(None, "fs", "tp"),
        P(None, "fs", "tp"),
        P(None, "fs", "tp"),
        P("fs", None),
        P("fs", None),
    )
    out_specs = (P("fs", "tp"), P("fs", None, "tp"), P("fs", None, "tp"), P("fs", None, "tp"))
    return jax.shard_map(body, mesh=mesh, in_specs=in_specs, out_specs=out_specs, check_vma=False)
```

```python
import functools

import jax
import jax.numpy as jnp
from jax import lax
from jax.experimental import pallas as pl
from jax.experimental.pallas import tpu as pltpu
from jax.sharding import PartitionSpec as P

epsilon = 1e-05


def slot_table(route, block_rows, expert_count):
    pair_ids = route.reshape(-1, block_rows * route.shape[1])
    onehot = (
        pair_ids[:, :, None] == jnp.arange(expert_count, dtype=jnp.int32)[None, None, :]
    ).astype(jnp.int32)
    before = jnp.cumsum(onehot, axis=1) - onehot
    return jnp.sum(before * onehot, axis=2).reshape(route.shape)


def slotted_body(tokens, norm_gain, gate_weight, up_weight, down_weight, route, route_weight):
    experts = gate_weight.shape[0]
    tok_rows = tokens.shape[0]
    columns = tokens.shape[1]
    fs_count = lax.axis_size("fs")
    capacity = 4 * tok_rows // fs_count
    gain_col = norm_gain[None, :, None]
    gate_cast = (gate_weight * gain_col).astype(jnp.bfloat16)
    up_cast = (up_weight * gain_col).astype(jnp.bfloat16)
    down_cast = down_weight.astype(jnp.bfloat16)
    gate_new, up_new, down_new = (
        lax.all_to_all(gate_cast, "fs", split_axis=0, concat_axis=1, tiled=True),
        lax.all_to_all(up_cast, "fs", split_axis=0, concat_axis=1, tiled=True),
        lax.all_to_all(down_cast, "fs", split_axis=0, concat_axis=1, tiled=True),
    )
    slot_of = slot_table(route, tok_rows, experts)
    target = route * capacity + slot_of
    slot_lanes = jnp.arange(experts * capacity, dtype=jnp.int32)
    slot_hits = target[:, :, None] == slot_lanes[None, None, :]
    token_iota = jnp.arange(tok_rows, dtype=jnp.int32)[:, None, None]
    lane_token = jnp.sum(jnp.where(slot_hits, token_iota + 1, 0), axis=(0, 1)) - 1
    lane_token = jnp.where(lane_token < 0, tok_rows, lane_token)
    combine = jnp.sum(jnp.where(slot_hits, route_weight[:, :, None], 0.0), axis=1)
    tok_float = tokens.astype(jnp.float32)
    square_sum = lax.psum(jnp.sum(tok_float * tok_float, axis=1), "tp")
    full_width = columns * lax.axis_size("tp")
    normed = (tok_float * lax.rsqrt(square_sum / full_width + epsilon)[:, None]).astype(
        jnp.bfloat16
    )
    padded = jnp.concatenate([normed, jnp.zeros((1, columns), jnp.bfloat16)], axis=0)
    outgoing = padded[lane_token].reshape(experts, capacity, columns)
    arrived = lax.all_to_all(outgoing, "fs", split_axis=0, concat_axis=0, tiled=True).reshape(
        -1, columns
    )
    gate_local = gate_new[0]
    up_local = up_new[0]
    piece_rows = lax.all_gather(arrived, "tp", axis=1, tiled=True)
    gate_acc = jnp.dot(piece_rows, gate_local, preferred_element_type=jnp.float32)
    up_acc = jnp.dot(piece_rows, up_local, preferred_element_type=jnp.float32)
    hidden = (jax.nn.silu(gate_acc) * up_acc).astype(jnp.bfloat16)
    down_local = down_new[0]
    summed = lax.psum_scatter(
        lax.dot_general(
            down_local, hidden, (((1,), (1,)), ((), ())), preferred_element_type=jnp.float32
        ).astype(jnp.bfloat16),
        "tp",
        scatter_dimension=0,
        tiled=True,
    ).astype(jnp.float32)
    own_columns = summed.shape[0]
    outgoing_back = summed.astype(jnp.bfloat16).reshape(own_columns, fs_count, capacity)
    returned = lax.all_to_all(outgoing_back, "fs", split_axis=1, concat_axis=1, tiled=True).reshape(
        own_columns, experts * capacity
    )
    mixed = lax.dot_general(
        combine,
        returned.astype(jnp.float32),
        (((1,), (1,)), ((), ())),
        precision=lax.Precision.HIGHEST,
        preferred_element_type=jnp.float32,
    )
    return (mixed.astype(jnp.bfloat16), gate_new, up_new, down_new)


MESH = pl.DeviceIdType.MESH
STAGES = 2
QUARTERS = 4
ISSUE = (1, 2, 3)
EXPECTED = (7.0, 13.5, 16.0, 19.0, 22.0, 24.0, 27.0, 30.5, 32.0)


def flip(index, distance):
    bit = 1
    while bit <= distance:
        if distance & bit:
            index = index + bit - 2 * bit * ((index // bit) % 2)
        bit *= 2
    return index


def plan(works, chain, bundle, chips):
    hop, pair = 4.7, 2.0
    starts, needs, now = [], [{}, {}], 0.0
    for w, (j, at, cost, sides) in enumerate(works):
        now = max(now, at)
        starts.append(now)
        now = now + cost
        for side in sides:
            needs[side][j] = (w, now)
    steps = [[[] for _ in range(chips)] for _ in works]
    before = {}
    for p in range(chips):
        side, leave, floor = 2 * p // chips, 0.0, 0
        for j in chain:
            w, done = max(needs[side][i] for i in needs[side] if bundle[i] == bundle[j])
            there = max(done + pair, before[j] + hop if p else 0.0)
            floor = max([floor, w] + [i for i, begin in enumerate(starts) if begin <= there])
            steps[floor][p].append(j)
            leave = max(leave + 1.0, there)
            before[j] = leave
    return steps


def rows_of(index, size):
    return pl.ds(pl.multiple_of(index * size, size), size)


def moe_kernel(
    fs,
    tp,
    tokens,
    gain,
    gate,
    up,
    down,
    route,
    route_weight,
    mixed,
    w_gate,
    w_up,
    w_down,
    gain_row,
    routes,
    weights_of,
    loaded,
    staged,
    tok,
    gated,
    up_acc,
    hidden,
    pair_own,
    pair_out,
    pair_in,
    chain_in,
    chain_out,
    back_in,
    share,
    mix_out,
    side_in,
    part_out,
    part_in,
    gain_col,
    load_sem,
    small_sem,
    tf_s,
    tf_r,
    az_s,
    az_r,
    as_s,
    as_r,
    w_s,
    g_r,
    u_r,
    dn_r,
    pr_s,
    pr_r,
    ch_s,
    ch_r,
    bk_s,
    bk_r,
    mx_s,
    mx_r,
    sd_s,
    sd_r,
    pt_s,
    pt_r,
):
    chips = tp // 2
    last = chips - 1
    f = lax.axis_index("fs")
    t = lax.axis_index("tp")
    z, core = t // 2, t % 2
    sibling = flip(t, 1)
    onward = t + 4 * core - 2
    place = core * z + (1 - core) * (last - z)
    hub = t - core + 1
    mixes = jnp.logical_and(core == 1, jnp.logical_or(z == 0, z == last))
    alone = jnp.logical_and(core == 1, z == last)
    strip, width = tokens.shape[1], tokens.shape[2]
    depth, units = gate.shape[1], gate.shape[2]
    block, rows_all = QUARTERS * strip, fs * QUARTERS * strip
    sub = width // STAGES
    piece_rows = fs * strip
    first = 1 - z // (chips // 2)
    sources, finals = (gate, up, down), (w_gate, w_up, w_down)

    barrier = pltpu.get_barrier_semaphore()
    for d in range(1, fs):
        pl.semaphore_signal(barrier, inc=1, device_id={"fs": flip(f, d)}, device_id_type=MESH)
        beyond = {"fs": flip(f, d), "tp": sibling}
        pl.semaphore_signal(barrier, inc=1, device_id=beyond, device_id_type=MESH)
    near = list(range(1, tp))
    for d in near:
        pl.semaphore_signal(barrier, inc=1, device_id={"tp": flip(t, d)}, device_id_type=MESH)

    def tok_at(k, d):
        return tok.at[k, :, flip(f, d)]

    small = [
        pltpu.make_async_copy(source, target, small_sem.at[n])
        for n, (source, target) in enumerate(
            (
                (tokens, tok_at(t, 0)),
                (gain, gain_row),
                (route, routes),
                (route_weight, weights_of),
            )
        )
    ]
    for copy in small:
        copy.start()
    def load(p, d):
        sem = load_sem.at[p if d else 3]
        pltpu.make_async_copy(sources[p].at[flip(f, d)], loaded.at[p, d], sem).start()

    for d in ISSUE:
        load(0, d)
    for copy in small:
        copy.wait()
    pl.semaphore_wait(barrier, 2 * (fs - 1) + len(near))

    def remote(src, dst, s_sem, r_sem, **device):
        return pltpu.make_async_remote_copy(
            src_ref=src,
            dst_ref=dst,
            send_sem=s_sem,
            recv_sem=r_sem,
            device_id=device,
            device_id_type=MESH,
        )

    def send(*args, **device):
        copy = remote(*args, **device)
        copy.start()
        return copy

    def send_if(condition, *args, **device):
        @pl.when(condition)
        def _():
            remote(*args, **device).start()

    def take(ref, sem):
        pltpu.make_async_copy(ref, ref, sem).wait()

    beside = ISSUE[:2]
    across = ISSUE[2]
    tok_fs = {
        d: send(tok_at(t, 0), tok_at(t, 0), tf_s, tf_r.at[d], fs=flip(f, d)) for d in beside
    }

    def tok_part(n, d):
        size = QUARTERS // 2
        return tok.at[t, pl.ds(n * size, size), flip(f, d)]

    def pass_on(n):
        piece = tok_part(n, beside[n])
        send(piece, piece, tf_s, tf_r.at[0 if n else across], fs=flip(f, beside[1 - n]))

    def spread(d):
        piece = tok_at(t, d)
        send_if(z < last, piece, piece, az_s.at[0], az_r.at[z, d], tp=t + 2)
        send_if(z > 0, piece, piece, az_s.at[1], az_r.at[z, d], tp=t - 2)
        send(piece, piece, as_s, as_r, tp=sibling)

    def relay(step, d):
        for way in range(2):
            towards = 1 - 2 * way
            here = (z >= step) if way == 0 else (z + step <= last)
            more = (z < last) if way == 0 else (z > 0)
            k = t - 2 * step * towards
            origin = z - step * towards
            piece = tok_at(k, d)

            @pl.when(here)
            def _():
                take(piece, az_r.at[origin, d])

            send_if(
                jnp.logical_and(here, more),
                piece,
                piece,
                az_s.at[way],
                az_r.at[origin, d],
                tp=t + 2 * towards,
            )
            send_if(here, piece, piece, as_s, as_r, tp=sibling)

    def cast(p, d):
        if d == ISSUE[0]:
            take(loaded.at[p, pl.ds(1, fs - 1)], load_sem.at[p])
        elif d == 0 and p == 0:
            take(loaded.at[:, 0], load_sem.at[3])
        tile = 64

        @pl.loop(0, depth // tile)
        def _(i):
            rows = rows_of(i, tile)
            value = loaded[p, d, rows, :]
            if p < 2:
                value = value * gain_col[rows, 0:1]
            value = value.astype(jnp.bfloat16)
            if d:
                staged[p, d - 1, rows, :] = value
            else:
                finals[p][pl.ds(pl.multiple_of(f * depth + i * tile, tile), tile), :] = value

    arrive = {}

    def ship(p, d):
        cast(p, d)
        arrive[p, d] = send(
            staged.at[p, d - 1],
            finals[p].at[rows_of(f, depth)],
            w_s,
            u_r.at[d - 1] if p else g_r,
            fs=flip(f, d),
        )

    spread(0)
    gain_col[...] = jnp.broadcast_to(gain_row[...], (128, depth)).T
    for d in ISSUE:
        load(1, d)
    for d in beside:
        ship(0, d)
    for d in ISSUE:
        load(2, d)
    for n, d in enumerate(beside):
        tok_fs[d].wait_recv()
        spread(d)
        pass_on(n)
    ship(0, across)
    for d in ISSUE:
        ship(1, d)
    for p in range(3):
        load(p, 0)
    for d in ISSUE:
        cast(2, d)
    def send_down(u, d, c, r_sem):
        send(
            staged.at[2, d - 1, pl.ds(pl.multiple_of(c * width + u * sub, sub), sub)],
            w_down.at[pl.ds(pl.multiple_of(f * depth + c * width + u * sub, sub), sub)],
            w_s,
            r_sem,
            fs=flip(f, d),
        )

    for u in range(STAGES - 1):
        for d in ISSUE:
            for c in range(2):
                send_down(u, d, c, dn_r.at[u, d - 1])
    for turn in range(2):
        for d in ISSUE:
            c = 1 - first if turn else first
            send_down(STAGES - 1, d, c, dn_r.at[STAGES - 1 + turn, d - 1])
    for step in range(1, chips):
        for d in (0,) + beside:
            relay(step, d)
        if step == 1:
            for p in range(3):
                cast(p, 0)
            for e in range(fs):
                part = jnp.zeros((1, block), jnp.float32)
                for k in range(routes.shape[0]):
                    part = part + jnp.where(
                        routes[k : k + 1, :] == e, weights_of[k : k + 1, :], 0.0
                    )
                share[e] = jnp.broadcast_to(part, (sub, block)).T
        if step == chips - 2:
            for n in range(2):
                take(tok_part(n, across), tf_r.at[0 if n else across])
            spread(across)
    for step in range(1, chips):
        relay(step, across)
    take(tok.at[pl.ds(0, chips)], as_r)
    take(w_gate.at[pl.ds(0, (fs - 1) * depth)], g_r)

    def tok_rows(k, i):
        return tok[k, i].reshape(piece_rows, width)

    @pl.loop(0, QUARTERS)
    def _(i):
        rows = rows_of(i, piece_rows)
        parts = [tok_rows(k, i) for k in range(tp)]
        squares = jnp.zeros((piece_rows, 1), jnp.float32)
        for part in parts:
            value = part.astype(jnp.float32)
            squares = squares + jnp.sum(value * value, axis=1, keepdims=True)
        scale = lax.rsqrt(squares / (width * tp) + epsilon)
        acc = jnp.dot(
            jnp.concatenate(parts, axis=1), w_gate[...], preferred_element_type=jnp.float32
        )
        gated[rows, :] = jax.nn.silu(acc * scale) * scale

    def up_part(d, i):
        s = flip(f, d)
        value = jnp.concatenate([tok_rows(2 * s, i), tok_rows(2 * s + 1, i)], axis=1)
        return jnp.dot(value, w_up[rows_of(s, depth), :], preferred_element_type=jnp.float32)

    early = (0,) + ISSUE[:-1]
    for n, d in enumerate(early):
        if d:
            arrive[1, d].wait_recv()

        @pl.loop(0, QUARTERS)
        def _(i):
            rows = rows_of(i, piece_rows)
            part = up_part(d, i)
            up_acc[rows, :] = up_acc[rows, :] + part if n else part

    arrive[1, ISSUE[-1]].wait_recv()

    def finish_hidden(h):
        rows = pl.ds(h * piece_rows, piece_rows)
        value = up_acc[rows, :] + up_part(ISSUE[-1], h)
        hidden[rows, :] = (gated[rows, :] * value).astype(jnp.bfloat16)

    end = STAGES - 1
    pieces = [(u, 0, h) for h in range(QUARTERS) for u in range(STAGES)]
    pieces += [(u, d, h) for u in range(STAGES) for d in ISSUE for h in range(QUARTERS)]
    count = len(pieces)
    late = QUARTERS - 1
    chain = [j for j, (u, _, h) in enumerate(pieces) if u < end or h < late]
    bundle, lead = {}, {}
    for j, (u, d, h) in enumerate(pieces):
        key = late if u == end and h == late else (u, d, h if d == 0 else h // 2 if u < end else 0)
        bundle[j] = lead.setdefault(key, (len(lead), j))[0]
    sizes = [list(bundle.values()).count(n) for n in range(len(lead))]
    leads = {j: n for n, j in lead.values()}

    def product(j, turn):
        u, d, h = pieces[j]
        s = flip(f, d)
        if d == 0 and u == 0:
            finish_hidden(h)
        if d and h == 0:
            size = 2 * sub if turn is None else sub
            take(w_down.at[pl.ds(0, size)], dn_r.at[u + (turn or 0), d - 1])

        def weights(c):
            start = pl.multiple_of(s * depth + c * width + u * sub, sub)
            return w_down[pl.ds(start, sub), :]

        def times(weight):
            return lax.dot_general(
                hidden[pl.ds(h * piece_rows, piece_rows), :],
                weight,
                (((1,), (1,)), ((), ())),
                preferred_element_type=jnp.float32,
            )

        def give(value):
            pair_out[j] = value.astype(jnp.bfloat16)
            send(pair_out.at[j], pair_in.at[j], pr_s, pr_r.at[bundle[j]], tp=sibling)

        if turn is None:
            result = times(jnp.concatenate([weights(core), weights(1 - core)], axis=0))
            pair_own[j] = result[:, :sub]
            give(result[:, sub:])
            return
        c = 1 - first if turn else first
        result = times(weights(c))

        @pl.when(core == c)
        def _():
            pair_own[j] = result

        @pl.when(core != c)
        def _():
            give(result)

    def advance(p, j):
        u, d, h = pieces[j]
        s = flip(f, d)
        if j in leads:
            take(pair_in.at[pl.ds(j, sizes[leads[j]])], pr_r.at[leads[j]])
        if p:
            take(chain_in.at[j], ch_r.at[j])

        value = pair_own[j] + pair_in[j].astype(jnp.float32)
        if p:
            value = value + chain_in[j].astype(jnp.float32)
        chain_out[j] = value.astype(jnp.bfloat16)

        if p < last:
            send(chain_out.at[j], chain_in.at[j], ch_s, ch_r.at[j], tp=onward)
            return
        for b in range(fs):
            rows = pl.ds(b * strip, strip)
            here = jnp.logical_and(f == b, core == 1)

            @pl.when(here)
            def _():
                back_in[u, h, s, f] = chain_out[j, rows, :]

            @pl.when(jnp.logical_not(here))
            def _():
                send(
                    chain_out.at[j, rows],
                    back_in.at[u, h, s, f],
                    bk_s,
                    bk_r.at[1 + h if u == end else u],
                    fs=b,
                    tp=hub,
                )

    def mix(shares, h):
        value = jnp.zeros((strip, sub), jnp.float32)
        for e in range(fs):
            rows = pl.ds(h * strip, strip)
            value = value + share[e, rows, :] * shares[e].astype(jnp.float32)
        return value.astype(jnp.bfloat16)

    def combine(u, h):
        @pl.when(alone)
        def _():
            if u == end:
                take(back_in.at[u, h, :, pl.ds(0, fs - 1)], bk_r.at[1 + h])
            elif h == 0:
                take(back_in.at[u, :, :, pl.ds(0, fs - 1)], bk_r.at[u])

        @pl.when(jnp.logical_not(alone))
        def _():
            if u == end:
                take(back_in.at[u, h], bk_r.at[1 + h])
            elif h == 0:
                take(back_in.at[u], bk_r.at[u])

        for s in range(fs):
            value = mix([back_in[u, h, s, e] for e in range(fs)], h)
            here = jnp.logical_and(s == z, alone)

            @pl.when(here)
            def _():
                mixed[u, h] = value

            @pl.when(jnp.logical_not(here))
            def _():
                mix_out[u, h, s] = value
                send(mix_out.at[u, h, s], mixed.at[u, h], mx_s, mx_r, tp=2 * s + z // last)

    def offer():
        for d in (0,) + ISSUE:
            j = index[end, d, late]
            s = flip(f, d)
            if d == 0:
                take(pair_in.at[pl.ds(0, sizes[bundle[j]])], pr_r.at[bundle[j]])
            value = pair_own[j] + pair_in[j].astype(jnp.float32)
            chain_out[j] = value.astype(jnp.bfloat16)
            for b in range(fs):
                rows = pl.ds(b * strip, strip)

                @pl.when(f != b)
                def _():
                    send(chain_out.at[j, rows], side_in.at[s, f], sd_s, sd_r, fs=b)

                @pl.when(f == b)
                def _():
                    side_in[s, f] = chain_out[j, rows, :]

    def settle():
        take(side_in.at[:, pl.ds(0, fs - 1)], sd_r)
        for s in range(fs):
            value = mix([side_in[s, e] for e in range(fs)], late)

            @pl.when(s == z)
            def _():
                part_in[s] = value

            @pl.when(s != z)
            def _():
                part_out[s] = value
                send(part_out.at[s], part_in.at[z], pt_s, pt_r, tp=2 * s + core)

    def close():
        take(part_in.at[pl.ds(0, chips - 1)], pt_r)
        value = jnp.zeros((strip, sub), jnp.float32)
        for k in range(chips):
            value = value + part_in[k].astype(jnp.float32)
        mixed[end, late] = value.astype(jnp.bfloat16)

    works = [(j, 0.0, 0.5 if pieces[j][0] else 1.0, (0, 1)) for j in range(STAGES * QUARTERS)]
    times_of = iter(EXPECTED)
    index = {piece: j for j, piece in enumerate(pieces)}
    for u in range(STAGES):
        for turn in (0, 1) if u == end else (None,):
            for d in ISSUE:
                at = next(times_of)
                turns = (0, 1) if turn is None else (turn,)
                works += [(index[u, d, h], at, 0.5, turns) for h in range(QUARTERS)]
    steps = plan(works, chain, bundle, chips)
    split = {j for j in range(count) if pieces[j][0] == end and pieces[j][1]}
    for w, (j, _, _, turns) in enumerate(works):
        product(j, turns[0] if j in split else None)
        for p in range(chips):
            todo = steps[w][p]
            if not todo and w < len(works) - 1:
                continue

            @pl.when(place == p)
            def _():
                for i in todo[:2]:
                    advance(p, i)
                if w == len(works) - 1:
                    offer()
                for i in todo[2:]:
                    advance(p, i)

    placed = [(u, h) for u in range(STAGES) for h in range(QUARTERS) if u < end or h < late]

    settle()

    @pl.when(mixes)
    def _():
        for u, h in placed:
            combine(u, h)

    close()
    @pl.when(jnp.logical_not(alone))
    def _():
        take(chain_out.at[pl.ds(0, len(placed)), pl.ds(0, strip)], mx_r)


    take(tok.at[0, :, pl.ds(0, fs - 1)], tf_s)
    for n in range(chips):

        @pl.when(z == n)
        def _():
            if n < last:
                take(tok.at[pl.ds(0, 1 + n)], az_s.at[0])
            if n:
                take(tok.at[pl.ds(0, chips - n)], az_s.at[1])

    take(tok.at[pl.ds(0, chips)], as_s)
    take(staged, w_s)
    take(pair_out, pr_s)

    take(side_in.at[:, pl.ds(0, fs - 1)], sd_s)
    take(part_out.at[pl.ds(0, chips - 1)], pt_s)
    passed = chain_out.at[pl.ds(0, len(chain))]

    @pl.when(place < last)
    def _():
        take(passed, ch_s)

    @pl.when(jnp.logical_and(place == last, core == 0))
    def _():
        take(passed, bk_s)

    @pl.when(jnp.logical_and(mixes, z == 0))
    def _():
        take(chain_out.at[pl.ds(0, len(placed))], mx_s)

    @pl.when(alone)
    def _():
        take(chain_out.at[pl.ds(0, len(chain)), pl.ds(0, (fs - 1) * strip)], bk_s)
        take(chain_out.at[pl.ds(0, len(placed)), pl.ds(0, (fs - 1) * strip)], mx_s)


def write_kernel(mixed, gate, up, down, mixed_out, gate_out, up_out, down_out, sem):
    sub = mixed.shape[3]
    copies = [
        pltpu.make_async_copy(mixed.at[u], mixed_out.at[:, :, pl.ds(u * sub, sub)], sem.at[u])
        for u in range(STAGES)
    ]
    pairs = ((gate, gate_out), (up, up_out), (down, down_out))
    copies += [
        pltpu.make_async_copy(source, target.at[0], sem.at[STAGES + n])
        for n, (source, target) in enumerate(pairs)
    ]
    for copy in copies:
        copy.start()
    for copy in copies:
        copy.wait()


def write_out(mixed, *weights):
    whole = pl.BlockSpec(memory_space=pltpu.VMEM)
    far = pl.BlockSpec(memory_space=pl.ANY)
    stages, quarters, strip, sub = mixed.shape
    shapes = [jax.ShapeDtypeStruct((quarters, strip, stages * sub), mixed.dtype)]
    shapes += [jax.ShapeDtypeStruct((1,) + w.shape, w.dtype) for w in weights]
    mixed, *weights = pl.pallas_call(
        write_kernel,
        out_shape=tuple(shapes),
        in_specs=[whole] * len(shapes),
        out_specs=tuple([far] * len(shapes)),
        scratch_shapes=[pltpu.SemaphoreType.DMA((stages + len(weights),))],
        compiler_params=pltpu.CompilerParams(vmem_limit_bytes=1024 * 1024),
    )(mixed, *weights)
    return (mixed.reshape(quarters * strip, stages * sub), *weights)


def dense_body(tokens, norm_gain, gate_weight, up_weight, down_weight, route, route_weight):
    fs, tp = lax.axis_size("fs"), lax.axis_size("tp")
    block, width = tokens.shape
    experts, depth, units = gate_weight.shape
    rows, full, sub, chips = fs * block, tp * width, width // STAGES, tp // 2
    count, strip = STAGES * fs * QUARTERS, block // QUARTERS
    piece = fs * strip
    whole = pl.BlockSpec(memory_space=pltpu.VMEM)
    far = pl.BlockSpec(memory_space=pl.ANY)
    narrow, wide, dma = jnp.bfloat16, jnp.float32, pltpu.SemaphoreType.DMA
    weight = pltpu.VMEM((full, units), narrow)
    mixed, gate_new, up_new, down_new = pl.pallas_call(
        functools.partial(moe_kernel, fs, tp),
        out_shape=(pltpu.VMEM((STAGES, QUARTERS, strip, sub), narrow), weight, weight, weight),
        in_specs=[far] * 7,
        out_specs=(whole, whole, whole, whole),
        scratch_shapes=[
            pltpu.VMEM((1, depth), wide),
            pltpu.VMEM((route.shape[1], block), jnp.int32),
            pltpu.VMEM((route.shape[1], block), wide),
            pltpu.VMEM((3, experts, depth, units), wide),
            pltpu.VMEM((3, fs - 1, depth, units), narrow),
            pltpu.VMEM((tp, QUARTERS, fs, strip, width), narrow),
            pltpu.VMEM((rows, units), wide),
            pltpu.VMEM((rows, units), wide),
            pltpu.VMEM((rows, units), narrow),
            pltpu.VMEM((count, piece, sub), wide),
            pltpu.VMEM((count, piece, sub), narrow),
            pltpu.VMEM((count, piece, sub), narrow),
            pltpu.VMEM((count, piece, sub), narrow),
            pltpu.VMEM((count, piece, sub), narrow),
            pltpu.VMEM((STAGES, QUARTERS, fs, fs, strip, sub), narrow),
            pltpu.VMEM((fs, block, sub), wide),
            pltpu.VMEM((STAGES, QUARTERS, fs, strip, sub), narrow),
            pltpu.VMEM((fs, fs, strip, sub), narrow),
            pltpu.VMEM((fs, strip, sub), narrow),
            pltpu.VMEM((chips, strip, sub), narrow),
            pltpu.VMEM((depth, 128), wide),
            dma((4,)),
            dma((4,)),
            dma,
            dma((fs,)),
            dma((2,)),
            dma((chips, fs)),
            dma,
            dma,
            dma,
            dma,
            dma((fs - 1,)),
            dma((STAGES + 1, fs - 1)),
            dma,
            dma((count // 2 + 1,)),
            dma,
            dma((count,)),
            dma,
            dma((QUARTERS + 1,)),
            dma,
            dma,
            dma,
            dma,
            dma,
            dma,
        ],
        compiler_params=pltpu.CompilerParams(
            collective_id=0, has_side_effects=True, vmem_limit_bytes=56 * 1024 * 1024
        ),
    )(
        tokens.reshape(QUARTERS, strip, width),
        norm_gain[None, :],
        gate_weight,
        up_weight,
        down_weight,
        route.T,
        route_weight.T,
    )
    return write_out(mixed, gate_new, up_new, down_new)


def body(tokens, norm_gain, gate_weight, up_weight, down_weight, route, route_weight):
    fs, tp = lax.axis_size("fs"), lax.axis_size("tp")
    fits = (
        fs == 4
        and tp == 2 * fs
        and gate_weight.shape[0] == fs
        and tokens.shape[1] % (128 * STAGES) == 0
        and tokens.shape[0] % (64 * QUARTERS) == 0
        and gate_weight.shape[1] == 2 * tokens.shape[1]
        and tokens.shape[0] * fs * tokens.shape[1] * tp <= 1024 * 2048
    )
    chosen = dense_body if fits else slotted_body
    return chosen(tokens, norm_gain, gate_weight, up_weight, down_weight, route, route_weight)


def solution(mesh):
    in_specs = (
        P("fs", "tp"),
        P("fs"),
        P(None, "fs", "tp"),
        P(None, "fs", "tp"),
        P(None, "fs", "tp"),
        P("fs", None),
        P("fs", None),
    )
    out_specs = (P("fs", "tp"), P("fs", None, "tp"), P("fs", None, "tp"), P("fs", None, "tp"))
    return jax.shard_map(body, mesh=mesh, in_specs=in_specs, out_specs=out_specs, check_vma=False)
```

```python
import functools

import jax
import jax.numpy as jnp
from jax import lax
from jax.experimental import pallas as pl
from jax.experimental.pallas import tpu as pltpu
from jax.sharding import PartitionSpec as P

epsilon = 1e-05


def slot_table(route, block_rows, expert_count):
    pair_ids = route.reshape(-1, block_rows * route.shape[1])
    onehot = (
        pair_ids[:, :, None] == jnp.arange(expert_count, dtype=jnp.int32)[None, None, :]
    ).astype(jnp.int32)
    before = jnp.cumsum(onehot, axis=1) - onehot
    return jnp.sum(before * onehot, axis=2).reshape(route.shape)


def slotted_body(tokens, norm_gain, gate_weight, up_weight, down_weight, route, route_weight):
    experts = gate_weight.shape[0]
    tok_rows = tokens.shape[0]
    columns = tokens.shape[1]
    fs_count = lax.axis_size("fs")
    capacity = 4 * tok_rows // fs_count
    gain_col = norm_gain[None, :, None]
    gate_cast = (gate_weight * gain_col).astype(jnp.bfloat16)
    up_cast = (up_weight * gain_col).astype(jnp.bfloat16)
    down_cast = down_weight.astype(jnp.bfloat16)
    gate_new, up_new, down_new = (
        lax.all_to_all(gate_cast, "fs", split_axis=0, concat_axis=1, tiled=True),
        lax.all_to_all(up_cast, "fs", split_axis=0, concat_axis=1, tiled=True),
        lax.all_to_all(down_cast, "fs", split_axis=0, concat_axis=1, tiled=True),
    )
    slot_of = slot_table(route, tok_rows, experts)
    target = route * capacity + slot_of
    slot_lanes = jnp.arange(experts * capacity, dtype=jnp.int32)
    slot_hits = target[:, :, None] == slot_lanes[None, None, :]
    token_iota = jnp.arange(tok_rows, dtype=jnp.int32)[:, None, None]
    lane_token = jnp.sum(jnp.where(slot_hits, token_iota + 1, 0), axis=(0, 1)) - 1
    lane_token = jnp.where(lane_token < 0, tok_rows, lane_token)
    combine = jnp.sum(jnp.where(slot_hits, route_weight[:, :, None], 0.0), axis=1)
    tok_float = tokens.astype(jnp.float32)
    square_sum = lax.psum(jnp.sum(tok_float * tok_float, axis=1), "tp")
    full_width = columns * lax.axis_size("tp")
    normed = (tok_float * lax.rsqrt(square_sum / full_width + epsilon)[:, None]).astype(
        jnp.bfloat16
    )
    padded = jnp.concatenate([normed, jnp.zeros((1, columns), jnp.bfloat16)], axis=0)
    outgoing = padded[lane_token].reshape(experts, capacity, columns)
    arrived = lax.all_to_all(outgoing, "fs", split_axis=0, concat_axis=0, tiled=True).reshape(
        -1, columns
    )
    gate_local = gate_new[0]
    up_local = up_new[0]
    piece_rows = lax.all_gather(arrived, "tp", axis=1, tiled=True)
    gate_acc = jnp.dot(piece_rows, gate_local, preferred_element_type=jnp.float32)
    up_acc = jnp.dot(piece_rows, up_local, preferred_element_type=jnp.float32)
    hidden = (jax.nn.silu(gate_acc) * up_acc).astype(jnp.bfloat16)
    down_local = down_new[0]
    summed = lax.psum_scatter(
        lax.dot_general(
            down_local, hidden, (((1,), (1,)), ((), ())), preferred_element_type=jnp.float32
        ).astype(jnp.bfloat16),
        "tp",
        scatter_dimension=0,
        tiled=True,
    ).astype(jnp.float32)
    own_columns = summed.shape[0]
    outgoing_back = summed.astype(jnp.bfloat16).reshape(own_columns, fs_count, capacity)
    returned = lax.all_to_all(outgoing_back, "fs", split_axis=1, concat_axis=1, tiled=True).reshape(
        own_columns, experts * capacity
    )
    mixed = lax.dot_general(
        combine,
        returned.astype(jnp.float32),
        (((1,), (1,)), ((), ())),
        precision=lax.Precision.HIGHEST,
        preferred_element_type=jnp.float32,
    )
    return (mixed.astype(jnp.bfloat16), gate_new, up_new, down_new)


MESH = pl.DeviceIdType.MESH
STAGES = 2
QUARTERS = 4
ISSUE = (1, 2, 3)
EXPECTED = (7.0, 12.0, 15.0, 18.0, 20.0, 22.0, 25.0, 28.0, 30.0)


def flip(index, distance):
    bit = 1
    while bit <= distance:
        if distance & bit:
            index = index + bit - 2 * bit * ((index // bit) % 2)
        bit *= 2
    return index


def plan(works, chain, bundle, chips):
    hop, pair = 4.0, 2.0
    starts, needs, now = [], [{}, {}], 0.0
    for w, (j, at, cost, sides) in enumerate(works):
        now = max(now, at)
        starts.append(now)
        now = now + cost
        for side in sides:
            needs[side][j] = (w, now)
    steps = [[[] for _ in range(chips)] for _ in works]
    before = {}
    for p in range(chips):
        side, leave, floor = 2 * p // chips, 0.0, 0
        for j in chain:
            w, done = max(needs[side][i] for i in needs[side] if bundle[i] == bundle[j])
            there = max(done + pair, before[j] + hop if p else 0.0)
            floor = max([floor, w] + [i for i, begin in enumerate(starts) if begin <= there])
            steps[floor][p].append(j)
            leave = max(leave + 1.0, there)
            before[j] = leave
    return steps


def rows_of(index, size):
    return pl.ds(pl.multiple_of(index * size, size), size)


def moe_kernel(
    fs,
    tp,
    tokens,
    gain,
    gate,
    up,
    down,
    route,
    route_weight,
    mixed,
    w_gate,
    w_up,
    w_down,
    gain_row,
    routes,
    weights_of,
    loaded,
    staged,
    tok,
    gated,
    up_acc,
    hidden,
    pair_own,
    pair_out,
    pair_in,
    chain_in,
    chain_out,
    back_in,
    share,
    mix_out,
    side_in,
    part_out,
    part_in,
    gain_col,
    load_sem,
    small_sem,
    tf_s,
    tf_r,
    az_s,
    az_r,
    as_s,
    as_r,
    w_s,
    g_r,
    u_r,
    dn_r,
    pr_s,
    pr_r,
    ch_s,
    ch_r,
    bk_s,
    bk_r,
    mx_s,
    mx_r,
    sd_s,
    sd_r,
    pt_s,
    pt_r,
):
    chips = tp // 2
    last = chips - 1
    f = lax.axis_index("fs")
    t = lax.axis_index("tp")
    z, core = t // 2, t % 2
    sibling = flip(t, 1)
    onward = t + 4 * core - 2
    place = core * z + (1 - core) * (last - z)
    hub = t - core + 1
    mixes = jnp.logical_and(core == 1, jnp.logical_or(z == 0, z == last))
    alone = jnp.logical_and(core == 1, z == last)
    strip, width = tokens.shape[1], tokens.shape[2]
    depth, units = gate.shape[1], gate.shape[2]
    block, rows_all = QUARTERS * strip, fs * QUARTERS * strip
    sub = width // STAGES
    piece_rows = fs * strip
    first = 1 - z // (chips // 2)
    sources, finals = (gate, up, down), (w_gate, w_up, w_down)

    barrier = pltpu.get_barrier_semaphore()
    for d in range(1, fs):
        pl.semaphore_signal(barrier, inc=1, device_id={"fs": flip(f, d)}, device_id_type=MESH)
        beyond = {"fs": flip(f, d), "tp": sibling}
        pl.semaphore_signal(barrier, inc=1, device_id=beyond, device_id_type=MESH)
    near = list(range(1, tp))
    for d in near:
        pl.semaphore_signal(barrier, inc=1, device_id={"tp": flip(t, d)}, device_id_type=MESH)

    def tok_at(k, d):
        return tok.at[k, :, flip(f, d)]

    small = [
        pltpu.make_async_copy(source, target, small_sem.at[n])
        for n, (source, target) in enumerate(
            (
                (tokens, tok_at(t, 0)),
                (gain, gain_row),
                (route, routes),
                (route_weight, weights_of),
            )
        )
    ]
    for copy in small:
        copy.start()
    def load(p, d):
        sem = load_sem.at[p if d else 3]
        pltpu.make_async_copy(sources[p].at[flip(f, d)], loaded.at[p, d], sem).start()

    for d in ISSUE:
        load(0, d)
    for copy in small:
        copy.wait()
    pl.semaphore_wait(barrier, 2 * (fs - 1) + len(near))

    def remote(src, dst, s_sem, r_sem, **device):
        return pltpu.make_async_remote_copy(
            src_ref=src,
            dst_ref=dst,
            send_sem=s_sem,
            recv_sem=r_sem,
            device_id=device,
            device_id_type=MESH,
        )

    def send(*args, **device):
        copy = remote(*args, **device)
        copy.start()
        return copy

    def send_if(condition, *args, **device):
        @pl.when(condition)
        def _():
            remote(*args, **device).start()

    def take(ref, sem):
        pltpu.make_async_copy(ref, ref, sem).wait()

    beside = ISSUE[:2]
    across = ISSUE[2]
    tok_fs = {
        d: send(tok_at(t, 0), tok_at(t, 0), tf_s, tf_r.at[d], fs=flip(f, d)) for d in beside
    }

    def tok_part(n, d):
        size = QUARTERS // 2
        return tok.at[t, pl.ds(n * size, size), flip(f, d)]

    def pass_on(n):
        piece = tok_part(n, beside[n])
        send(piece, piece, tf_s, tf_r.at[0 if n else across], fs=flip(f, beside[1 - n]))

    def spread(d):
        piece = tok_at(t, d)
        send_if(z < last, piece, piece, az_s.at[0], az_r.at[z, d], tp=t + 2)
        send_if(z > 0, piece, piece, az_s.at[1], az_r.at[z, d], tp=t - 2)
        send(piece, piece, as_s, as_r, tp=sibling)

    def relay(step, d):
        for way in range(2):
            towards = 1 - 2 * way
            here = (z >= step) if way == 0 else (z + step <= last)
            more = (z < last) if way == 0 else (z > 0)
            k = t - 2 * step * towards
            origin = z - step * towards
            piece = tok_at(k, d)

            @pl.when(here)
            def _():
                take(piece, az_r.at[origin, d])

            send_if(
                jnp.logical_and(here, more),
                piece,
                piece,
                az_s.at[way],
                az_r.at[origin, d],
                tp=t + 2 * towards,
            )
            send_if(here, piece, piece, as_s, as_r, tp=sibling)

    def cast(p, d):
        if d == ISSUE[0]:
            take(loaded.at[p, pl.ds(1, fs - 1)], load_sem.at[p])
        elif d == 0 and p == 0:
            take(loaded.at[:, 0], load_sem.at[3])
        tile = 64

        @pl.loop(0, depth // tile)
        def _(i):
            rows = rows_of(i, tile)
            value = loaded[p, d, rows, :]
            if p < 2:
                value = value * gain_col[rows, 0:1]
            value = value.astype(jnp.bfloat16)
            if d:
                staged[p, d - 1, rows, :] = value
            else:
                finals[p][pl.ds(pl.multiple_of(f * depth + i * tile, tile), tile), :] = value

    arrive = {}

    def ship(p, d):
        cast(p, d)
        arrive[p, d] = send(
            staged.at[p, d - 1],
            finals[p].at[rows_of(f, depth)],
            w_s,
            u_r.at[d - 1] if p else g_r,
            fs=flip(f, d),
        )

    spread(0)
    gain_col[...] = jnp.broadcast_to(gain_row[...], (128, depth)).T
    for d in ISSUE:
        load(1, d)
    for d in beside:
        ship(0, d)
    for d in ISSUE:
        load(2, d)
    for n, d in enumerate(beside):
        tok_fs[d].wait_recv()
        spread(d)
        pass_on(n)
    ship(0, across)
    for d in ISSUE:
        ship(1, d)
    for p in range(3):
        load(p, 0)
    for d in ISSUE:
        cast(2, d)
    def send_down(u, d, c, r_sem):
        send(
            staged.at[2, d - 1, pl.ds(pl.multiple_of(c * width + u * sub, sub), sub)],
            w_down.at[pl.ds(pl.multiple_of(f * depth + c * width + u * sub, sub), sub)],
            w_s,
            r_sem,
            fs=flip(f, d),
        )

    for u in range(STAGES - 1):
        for d in ISSUE:
            for c in range(2):
                send_down(u, d, c, dn_r.at[u, d - 1])
    for turn in range(2):
        for d in ISSUE:
            c = 1 - first if turn else first
            send_down(STAGES - 1, d, c, dn_r.at[STAGES - 1 + turn, d - 1])
    for step in range(1, chips):
        for d in (0,) + beside:
            relay(step, d)
        if step == 1:
            for p in range(3):
                cast(p, 0)
            for e in range(fs):
                part = jnp.zeros((1, block), jnp.float32)
                for k in range(routes.shape[0]):
                    part = part + jnp.where(
                        routes[k : k + 1, :] == e, weights_of[k : k + 1, :], 0.0
                    )
                share[e] = jnp.broadcast_to(part, (sub, block)).T
        if step == chips - 2:
            for n in range(2):
                take(tok_part(n, across), tf_r.at[0 if n else across])
            spread(across)
    for step in range(1, chips):
        relay(step, across)
    take(tok.at[pl.ds(0, chips)], as_r)
    take(w_gate.at[pl.ds(0, (fs - 1) * depth)], g_r)

    def tok_rows(k, i):
        return tok[k, i].reshape(piece_rows, width)

    @pl.loop(0, QUARTERS)
    def _(i):
        rows = rows_of(i, piece_rows)
        parts = [tok_rows(k, i) for k in range(tp)]
        squares = jnp.zeros((piece_rows, 1), jnp.float32)
        for part in parts:
            value = part.astype(jnp.float32)
            squares = squares + jnp.sum(value * value, axis=1, keepdims=True)
        scale = lax.rsqrt(squares / (width * tp) + epsilon)
        acc = jnp.dot(
            jnp.concatenate(parts, axis=1), w_gate[...], preferred_element_type=jnp.float32
        )
        gated[rows, :] = jax.nn.silu(acc * scale) * scale

    def up_part(d, i):
        s = flip(f, d)
        value = jnp.concatenate([tok_rows(2 * s, i), tok_rows(2 * s + 1, i)], axis=1)
        return jnp.dot(value, w_up[rows_of(s, depth), :], preferred_element_type=jnp.float32)

    early = (0,) + ISSUE[:-1]
    for n, d in enumerate(early):
        if d:
            arrive[1, d].wait_recv()

        @pl.loop(0, QUARTERS)
        def _(i):
            rows = rows_of(i, piece_rows)
            part = up_part(d, i)
            up_acc[rows, :] = up_acc[rows, :] + part if n else part

    arrive[1, ISSUE[-1]].wait_recv()

    def finish_hidden(h):
        rows = pl.ds(h * piece_rows, piece_rows)
        value = up_acc[rows, :] + up_part(ISSUE[-1], h)
        hidden[rows, :] = (gated[rows, :] * value).astype(jnp.bfloat16)

    end = STAGES - 1
    pieces = [(u, 0, h) for h in range(QUARTERS) for u in range(STAGES)]
    pieces += [(u, d, h) for u in range(STAGES) for d in ISSUE for h in range(QUARTERS)]
    count = len(pieces)
    late = QUARTERS - 1
    chain = [j for j, (u, _, h) in enumerate(pieces) if u < end or h < late]
    bundle, lead = {}, {}
    for j, (u, d, h) in enumerate(pieces):
        key = late if u == end and h == late else (u, d, h if d == 0 else h // 2 if u < end else 0)
        bundle[j] = lead.setdefault(key, (len(lead), j))[0]
    sizes = [list(bundle.values()).count(n) for n in range(len(lead))]
    leads = {j: n for n, j in lead.values()}

    def product(j, turn):
        u, d, h = pieces[j]
        s = flip(f, d)
        if d == 0 and u == 0:
            finish_hidden(h)
        if d and h == 0:
            size = 2 * sub if turn is None else sub
            take(w_down.at[pl.ds(0, size)], dn_r.at[u + (turn or 0), d - 1])

        def weights(c):
            start = pl.multiple_of(s * depth + c * width + u * sub, sub)
            return w_down[pl.ds(start, sub), :]

        def times(weight):
            return lax.dot_general(
                hidden[pl.ds(h * piece_rows, piece_rows), :],
                weight,
                (((1,), (1,)), ((), ())),
                preferred_element_type=jnp.float32,
            )

        def give(value):
            pair_out[j] = value.astype(jnp.bfloat16)
            send(pair_out.at[j], pair_in.at[j], pr_s, pr_r.at[bundle[j]], tp=sibling)

        if turn is None:
            result = times(jnp.concatenate([weights(core), weights(1 - core)], axis=0))
            pair_own[j] = result[:, :sub]
            give(result[:, sub:])
            return
        c = 1 - first if turn else first
        result = times(weights(c))

        @pl.when(core == c)
        def _():
            pair_own[j] = result

        @pl.when(core != c)
        def _():
            give(result)

    def advance(p, j):
        u, d, h = pieces[j]
        s = flip(f, d)
        if j in leads:
            take(pair_in.at[pl.ds(j, sizes[leads[j]])], pr_r.at[leads[j]])
        if p:
            take(chain_in.at[j], ch_r.at[j])

        value = pair_own[j] + pair_in[j].astype(jnp.float32)
        if p:
            value = value + chain_in[j].astype(jnp.float32)
        chain_out[j] = value.astype(jnp.bfloat16)

        if p < last:
            send(chain_out.at[j], chain_in.at[j], ch_s, ch_r.at[j], tp=onward)
            return
        for b in range(fs):
            rows = pl.ds(b * strip, strip)
            here = jnp.logical_and(f == b, core == 1)

            @pl.when(here)
            def _():
                back_in[u, h, s, f] = chain_out[j, rows, :]

            @pl.when(jnp.logical_not(here))
            def _():
                send(
                    chain_out.at[j, rows],
                    back_in.at[u, h, s, f],
                    bk_s,
                    bk_r.at[1 + h if u == end else u],
                    fs=b,
                    tp=hub,
                )

    def mix(shares, h):
        value = jnp.zeros((strip, sub), jnp.float32)
        for e in range(fs):
            rows = pl.ds(h * strip, strip)
            value = value + share[e, rows, :] * shares[e].astype(jnp.float32)
        return value.astype(jnp.bfloat16)

    def combine(u, h):
        @pl.when(alone)
        def _():
            if u == end:
                take(back_in.at[u, h, :, pl.ds(0, fs - 1)], bk_r.at[1 + h])
            elif h == 0:
                take(back_in.at[u, :, :, pl.ds(0, fs - 1)], bk_r.at[u])

        @pl.when(jnp.logical_not(alone))
        def _():
            if u == end:
                take(back_in.at[u, h], bk_r.at[1 + h])
            elif h == 0:
                take(back_in.at[u], bk_r.at[u])

        for s in range(fs):
            value = mix([back_in[u, h, s, e] for e in range(fs)], h)
            here = jnp.logical_and(s == z, alone)

            @pl.when(here)
            def _():
                mixed[u, h] = value

            @pl.when(jnp.logical_not(here))
            def _():
                mix_out[u, h, s] = value
                send(mix_out.at[u, h, s], mixed.at[u, h], mx_s, mx_r, tp=2 * s + z // last)

    def offer():
        for d in (0,) + ISSUE:
            j = index[end, d, late]
            s = flip(f, d)
            if d == 0:
                take(pair_in.at[pl.ds(0, sizes[bundle[j]])], pr_r.at[bundle[j]])
            value = pair_own[j] + pair_in[j].astype(jnp.float32)
            chain_out[j] = value.astype(jnp.bfloat16)
            for b in range(fs):
                rows = pl.ds(b * strip, strip)

                @pl.when(f != b)
                def _():
                    send(chain_out.at[j, rows], side_in.at[s, f], sd_s, sd_r, fs=b)

                @pl.when(f == b)
                def _():
                    side_in[s, f] = chain_out[j, rows, :]

    def settle():
        take(side_in.at[:, pl.ds(0, fs - 1)], sd_r)
        for s in range(fs):
            value = mix([side_in[s, e] for e in range(fs)], late)

            @pl.when(s == z)
            def _():
                part_in[s] = value

            @pl.when(s != z)
            def _():
                part_out[s] = value
                send(part_out.at[s], part_in.at[z], pt_s, pt_r, tp=2 * s + core)

    def close():
        take(part_in.at[pl.ds(0, chips - 1)], pt_r)
        value = jnp.zeros((strip, sub), jnp.float32)
        for k in range(chips):
            value = value + part_in[k].astype(jnp.float32)
        mixed[end, late] = value.astype(jnp.bfloat16)

    works = [(j, 0.0, 0.5 if pieces[j][0] else 1.0, (0, 1)) for j in range(STAGES * QUARTERS)]
    times_of = iter(EXPECTED)
    index = {piece: j for j, piece in enumerate(pieces)}
    for u in range(STAGES):
        for turn in (0, 1) if u == end else (None,):
            for d in ISSUE:
                at = next(times_of)
                turns = (0, 1) if turn is None else (turn,)
                works += [(index[u, d, h], at, 0.5, turns) for h in range(QUARTERS)]
    steps = plan(works, chain, bundle, chips)
    split = {j for j in range(count) if pieces[j][0] == end and pieces[j][1]}
    for w, (j, _, _, turns) in enumerate(works):
        product(j, turns[0] if j in split else None)
        for p in range(chips):
            todo = steps[w][p]
            if not todo and w < len(works) - 1:
                continue

            @pl.when(place == p)
            def _():
                for i in todo[:2]:
                    advance(p, i)
                if w == len(works) - 1:
                    offer()
                for i in todo[2:]:
                    advance(p, i)

    placed = [(u, h) for u in range(STAGES) for h in range(QUARTERS) if u < end or h < late]

    settle()

    @pl.when(mixes)
    def _():
        for u, h in placed:
            combine(u, h)

    close()
    @pl.when(jnp.logical_not(alone))
    def _():
        take(chain_out.at[pl.ds(0, len(placed)), pl.ds(0, strip)], mx_r)


    take(tok.at[0, :, pl.ds(0, fs - 1)], tf_s)
    for n in range(chips):

        @pl.when(z == n)
        def _():
            if n < last:
                take(tok.at[pl.ds(0, 1 + n)], az_s.at[0])
            if n:
                take(tok.at[pl.ds(0, chips - n)], az_s.at[1])

    take(tok.at[pl.ds(0, chips)], as_s)
    take(staged, w_s)
    take(pair_out, pr_s)

    take(side_in.at[:, pl.ds(0, fs - 1)], sd_s)
    take(part_out.at[pl.ds(0, chips - 1)], pt_s)
    passed = chain_out.at[pl.ds(0, len(chain))]

    @pl.when(place < last)
    def _():
        take(passed, ch_s)

    @pl.when(jnp.logical_and(place == last, core == 0))
    def _():
        take(passed, bk_s)

    @pl.when(jnp.logical_and(mixes, z == 0))
    def _():
        take(chain_out.at[pl.ds(0, len(placed))], mx_s)

    @pl.when(alone)
    def _():
        take(chain_out.at[pl.ds(0, len(chain)), pl.ds(0, (fs - 1) * strip)], bk_s)
        take(chain_out.at[pl.ds(0, len(placed)), pl.ds(0, (fs - 1) * strip)], mx_s)


def write_kernel(mixed, gate, up, down, mixed_out, gate_out, up_out, down_out, sem):
    sub = mixed.shape[3]
    copies = [
        pltpu.make_async_copy(mixed.at[u], mixed_out.at[:, :, pl.ds(u * sub, sub)], sem.at[u])
        for u in range(STAGES)
    ]
    pairs = ((gate, gate_out), (up, up_out), (down, down_out))
    copies += [
        pltpu.make_async_copy(source, target.at[0], sem.at[STAGES + n])
        for n, (source, target) in enumerate(pairs)
    ]
    for copy in copies:
        copy.start()
    for copy in copies:
        copy.wait()


def write_out(mixed, *weights):
    whole = pl.BlockSpec(memory_space=pltpu.VMEM)
    far = pl.BlockSpec(memory_space=pl.ANY)
    stages, quarters, strip, sub = mixed.shape
    shapes = [jax.ShapeDtypeStruct((quarters, strip, stages * sub), mixed.dtype)]
    shapes += [jax.ShapeDtypeStruct((1,) + w.shape, w.dtype) for w in weights]
    mixed, *weights = pl.pallas_call(
        write_kernel,
        out_shape=tuple(shapes),
        in_specs=[whole] * len(shapes),
        out_specs=tuple([far] * len(shapes)),
        scratch_shapes=[pltpu.SemaphoreType.DMA((stages + len(weights),))],
        compiler_params=pltpu.CompilerParams(vmem_limit_bytes=1024 * 1024),
    )(mixed, *weights)
    return (mixed.reshape(quarters * strip, stages * sub), *weights)


def dense_body(tokens, norm_gain, gate_weight, up_weight, down_weight, route, route_weight):
    fs, tp = lax.axis_size("fs"), lax.axis_size("tp")
    block, width = tokens.shape
    experts, depth, units = gate_weight.shape
    rows, full, sub, chips = fs * block, tp * width, width // STAGES, tp // 2
    count, strip = STAGES * fs * QUARTERS, block // QUARTERS
    piece = fs * strip
    whole = pl.BlockSpec(memory_space=pltpu.VMEM)
    far = pl.BlockSpec(memory_space=pl.ANY)
    narrow, wide, dma = jnp.bfloat16, jnp.float32, pltpu.SemaphoreType.DMA
    weight = pltpu.VMEM((full, units), narrow)
    mixed, gate_new, up_new, down_new = pl.pallas_call(
        functools.partial(moe_kernel, fs, tp),
        out_shape=(pltpu.VMEM((STAGES, QUARTERS, strip, sub), narrow), weight, weight, weight),
        in_specs=[far] * 7,
        out_specs=(whole, whole, whole, whole),
        scratch_shapes=[
            pltpu.VMEM((1, depth), wide),
            pltpu.VMEM((route.shape[1], block), jnp.int32),
            pltpu.VMEM((route.shape[1], block), wide),
            pltpu.VMEM((3, experts, depth, units), wide),
            pltpu.VMEM((3, fs - 1, depth, units), narrow),
            pltpu.VMEM((tp, QUARTERS, fs, strip, width), narrow),
            pltpu.VMEM((rows, units), wide),
            pltpu.VMEM((rows, units), wide),
            pltpu.VMEM((rows, units), narrow),
            pltpu.VMEM((count, piece, sub), wide),
            pltpu.VMEM((count, piece, sub), narrow),
            pltpu.VMEM((count, piece, sub), narrow),
            pltpu.VMEM((count, piece, sub), narrow),
            pltpu.VMEM((count, piece, sub), narrow),
            pltpu.VMEM((STAGES, QUARTERS, fs, fs, strip, sub), narrow),
            pltpu.VMEM((fs, block, sub), wide),
            pltpu.VMEM((STAGES, QUARTERS, fs, strip, sub), narrow),
            pltpu.VMEM((fs, fs, strip, sub), narrow),
            pltpu.VMEM((fs, strip, sub), narrow),
            pltpu.VMEM((chips, strip, sub), narrow),
            pltpu.VMEM((depth, 128), wide),
            dma((4,)),
            dma((4,)),
            dma,
            dma((fs,)),
            dma((2,)),
            dma((chips, fs)),
            dma,
            dma,
            dma,
            dma,
            dma((fs - 1,)),
            dma((STAGES + 1, fs - 1)),
            dma,
            dma((count // 2 + 1,)),
            dma,
            dma((count,)),
            dma,
            dma((QUARTERS + 1,)),
            dma,
            dma,
            dma,
            dma,
            dma,
            dma,
        ],
        compiler_params=pltpu.CompilerParams(
            collective_id=0, has_side_effects=True, vmem_limit_bytes=56 * 1024 * 1024
        ),
    )(
        tokens.reshape(QUARTERS, strip, width),
        norm_gain[None, :],
        gate_weight,
        up_weight,
        down_weight,
        route.T,
        route_weight.T,
    )
    return write_out(mixed, gate_new, up_new, down_new)


def body(tokens, norm_gain, gate_weight, up_weight, down_weight, route, route_weight):
    fs, tp = lax.axis_size("fs"), lax.axis_size("tp")
    fits = (
        fs == 4
        and tp == 2 * fs
        and gate_weight.shape[0] == fs
        and tokens.shape[1] % (128 * STAGES) == 0
        and tokens.shape[0] % (64 * QUARTERS) == 0
        and gate_weight.shape[1] == 2 * tokens.shape[1]
        and tokens.shape[0] * fs * tokens.shape[1] * tp <= 1024 * 2048
    )
    chosen = dense_body if fits else slotted_body
    return chosen(tokens, norm_gain, gate_weight, up_weight, down_weight, route, route_weight)


def solution(mesh):
    in_specs = (
        P("fs", "tp"),
        P("fs"),
        P(None, "fs", "tp"),
        P(None, "fs", "tp"),
        P(None, "fs", "tp"),
        P("fs", None),
        P("fs", None),
    )
    out_specs = (P("fs", "tp"), P("fs", None, "tp"), P("fs", None, "tp"), P("fs", None, "tp"))
    return jax.shard_map(body, mesh=mesh, in_specs=in_specs, out_specs=out_specs, check_vma=False)
```
